32 devices in a mesh: sp: 8 (over z, y), tp: 4 (over x, core).
Axes of the slice: x: 2, y: 2, z: 4, core: 2. Of those that a mesh axis runs over, the one named last changes fastest.
Arguments:
- q_proj: bfloat16 [4096, 1024], P('sp', 'tp'), may hold values from -5.25 to 5.25
- k_proj: bfloat16 [4096, 512], P('sp', 'tp'), may hold values from -5.25 to 5.25
- v_proj: bfloat16 [4096, 512], P('sp', 'tp'), may hold values from -6 to 6
- doc_ids: int32 [4096], P('sp'), may hold values from 0 to 3, never falling along the last dimension, each value on 1 to 2048 neighbouring positions
- sinks: float32 [16], P('tp'), may hold values from 0.5 to 5.5
- resid: bfloat16 [4096, 2048], P(('sp', 'tp')), may hold values from -12 to 12
- w_out: bfloat16 [1024, 2048], P('tp'), may hold values from -4 to 4
- norm_gain: float32 [2048], replicated, may hold values from 0.1 to 1.9
- w_gate: bfloat16 [2048, 5632], P('sp', 'tp'), may hold values from -0.125 to 0.125
- w_up: bfloat16 [2048, 5632], P('sp', 'tp'), may hold values from -0.125 to 0.125
- w_down: bfloat16 [5632, 2048], P('tp', 'sp'), may hold values from -0.078125 to 0.078125
Outputs:
- layer_out: bfloat16 [4096, 2048], P(('sp', 'tp'))
The draws below stay inside these ranges and needn't reach their ends.
Inputs may be any that keep to these rules, and one draw needn't show every extreme that they name: `doc_ids`: document numbers never fall along the sequence; each document covers at most 2048 positions and one covers exactly that many.
All inputs are finite; a program needn't handle non-finite values.
Results may differ from the reference program's by a relative error of at most 0.015.
Values may be sent and summed in bfloat16 or wider, within the bound.
No kernel may reach another device: no remote copies, remote signals or barrier semaphores. Data moves between devices by JAX's collectives and lax.ppermute only.
A program may use at most 64 MiB of HBM per device.

```python
import math
import jax
import jax.numpy as jnp
import numpy as np
from jax import lax

D = 2048
HEADS = 16
KV_HEADS = 8
HEAD = 64
FF = 5632
WINDOW = 128
TOK_DEV = 512
TOKENS = 4096
DOCS = 4
DOC_MOST = 2048
N_SP = 8
N_TP = 4


def draw_k_proj(key, part):
    base = jnp.clip(jax.random.normal(jax.random.fold_in(key, 3), (TOKENS, KV_HEADS * HEAD), jnp.float32), -5.0, 5.0)
    return base.astype(jnp.bfloat16)


def draw_q_proj(key, part):
    base = jnp.clip(jax.random.normal(jax.random.fold_in(key, 5), (TOKENS, HEADS * HEAD), jnp.float32), -5.0, 5.0)
    return base.astype(jnp.bfloat16)


def draw_resid(key, part):
    block_total = D // 32
    scales = jnp.exp(jax.random.uniform(jax.random.fold_in(key, 21), (block_total,), jnp.float32, math.log(0.3), math.log(3.0)))
    column_scales = jnp.repeat(scales, 32)
    base = jnp.clip(jax.random.normal(jax.random.fold_in(key, 23), (TOKENS, D), jnp.float32), -4.0, 4.0)
    return (base * column_scales[None, :]).astype(jnp.bfloat16)


def block_scale(own_key, dims, shards, low, largest):
    level, own = 1.0, jax.random.fold_in(own_key, 6)
    for position, shards_of in shards:
        steps = jnp.exp(jax.random.uniform(jax.random.fold_in(own, position), (shards_of,), jnp.float32, low / len(shards), largest / len(shards)))
        level = level * jnp.repeat(steps, dims[position] // shards_of).reshape([-1 if axis == position else 1 for axis in range(len(dims))])
    return level


def split_up(amount, total, most, slope):
    loads = [(1 << 20) // math.isqrt(standing ** slope) + 1 for standing in range(2, amount + 1)]
    surplus, holding = total - most - (amount - 1), [1] * (amount - 1)
    while surplus > 0:
        candidates = [i for i in range(amount - 1) if holding[i] < most]
        mass, remaining = sum([loads[i] for i in candidates]), surplus
        for i in candidates:
            addition = min(most - holding[i], max(1, remaining * loads[i] // mass), surplus)
            holding[i] = holding[i] + addition
            surplus = surplus - addition
    return np.array([most] + holding)


def ragged(own_key, number_of, total, most, slope):
    if number_of == 2:
        one = jax.random.randint(own_key, (), max(1, total - most), min(most, total - 1) + 1)
        return jnp.stack([one, total - one])
    lengths = jnp.asarray(split_up(number_of, total, most, slope), jnp.int32)
    couples = (number_of - 1) // 2
    donor, taker = lengths[1:1 + 2 * couples:2], lengths[2:2 + 2 * couples:2]
    margin = jnp.minimum(donor - 1, most - taker)
    shifted = jax.random.randint(jax.random.fold_in(own_key, 1), (couples,), 0, 1 << 20) % (margin + 1)
    lengths = lengths.at[1:1 + 2 * couples:2].set(donor - shifted).at[2:2 + 2 * couples:2].set(taker + shifted)
    return lengths[jax.random.permutation(jax.random.fold_in(own_key, 2), number_of)]


def gaussian(own_key, dims, deviation, bound, shards=(), held_as=jnp.bfloat16):
    entries = jax.random.normal(own_key, dims, jnp.float32) * deviation
    if len(shards) > 0:
        entries = block_scale(own_key, dims, shards, -0.22, 0.18) * entries
    return jnp.clip(entries, min=-bound, max=bound).astype(held_as)


def setup_inputs(seed: int = 0) -> dict:
    key_list = jax.random.split(jax.random.key(seed), 12)
    q_proj = draw_q_proj(jax.random.fold_in(key_list[11], 71), 0)
    k_proj = draw_k_proj(jax.random.fold_in(key_list[11], 71), 0)
    v_proj = gaussian(key_list[2], (TOKENS, KV_HEADS * HEAD), 1.0, 6.0, ((0, 8), (1, 4)))
    doc_ids = jnp.searchsorted(jnp.cumsum(ragged(key_list[3], DOCS, TOKENS, DOC_MOST, 2)), jnp.arange(TOKENS), side="right").astype(jnp.int32)
    sinks = jnp.clip(0.5 + 5.0 * jax.random.uniform(key_list[4], (HEADS,), jnp.float32) ** block_scale(key_list[4], (HEADS,), ((0, 4),), -0.2, 0.2), 0.5, 5.5)
    resid = draw_resid(jax.random.fold_in(key_list[11], 71), 0)
    w_out = gaussian(key_list[6], (HEADS * HEAD, D), 0.25, 4.0, ((0, 4),))
    norm_gain = jnp.clip(1.0 + 0.18 * jax.random.normal(key_list[7], (D,), jnp.float32), 0.1, 1.9)
    w_gate = gaussian(key_list[8], (D, FF), D ** -0.5, 0.125, ((0, 8), (1, 4)))
    w_up = gaussian(key_list[9], (D, FF), D ** -0.5, 0.125, ((0, 8), (1, 4)))
    w_down = gaussian(key_list[10], (FF, D), FF ** -0.5, 0.078125, ((0, 4), (1, 8)))
    return {"q_proj": q_proj, "k_proj": k_proj, "v_proj": v_proj, "doc_ids": doc_ids, "sinks": sinks, "resid": resid, "w_out": w_out, "norm_gain": norm_gain, "w_gate": w_gate, "w_up": w_up, "w_down": w_down}


norm_eps = 1e-06
masked = -1e+30

def reference(q_proj, k_proj, v_proj, doc_ids, sinks, resid, w_out, norm_gain, w_gate, w_up, w_down):
    groups = HEADS // KV_HEADS
    block_count = TOKENS // WINDOW
    scale = HEAD ** (-0.5)
    padding = jnp.zeros((WINDOW, KV_HEADS * HEAD), jnp.bfloat16)
    keys_pad = jnp.concatenate([padding, k_proj, padding], axis=0)
    values_pad = jnp.concatenate([padding, v_proj, padding], axis=0)
    edge_docs = jnp.full((WINDOW,), -1, jnp.int32)
    docs_pad = jnp.concatenate([edge_docs, doc_ids.astype(jnp.int32), edge_docs], axis=0)
    offsets = jnp.arange(3 * WINDOW, dtype=jnp.int32) - WINDOW
    near = jnp.abs(jnp.arange(WINDOW, dtype=jnp.int32)[:, None] - offsets[None, :]) <= WINDOW
    sink_table = sinks.reshape(KV_HEADS, groups)[:, :, None, None]

    def attend_block(index):
        first = (index * WINDOW).astype(jnp.int32)
        queries = lax.dynamic_slice_in_dim(q_proj, first, WINDOW, 0).astype(jnp.float32).reshape(WINDOW, KV_HEADS, groups, HEAD)
        keys = lax.dynamic_slice_in_dim(keys_pad, first, 3 * WINDOW, 0).astype(jnp.float32).reshape(3 * WINDOW, KV_HEADS, HEAD)
        values = lax.dynamic_slice_in_dim(values_pad, first, 3 * WINDOW, 0).astype(jnp.float32).reshape(3 * WINDOW, KV_HEADS, HEAD)
        key_docs = lax.dynamic_slice_in_dim(docs_pad, first, 3 * WINDOW, 0)
        query_docs = lax.dynamic_slice_in_dim(doc_ids.astype(jnp.int32), first, WINDOW, 0)
        valid = near & (query_docs[:, None] == key_docs[None, :])
        scores = jnp.einsum('qhgd,khd->hgqk', queries, keys) * scale
        scores = jnp.where(valid[None, None], scores, masked)
        top = jnp.maximum(lax.optimization_barrier(jnp.max(scores, axis=-1, keepdims=True)), sink_table)
        expd = jnp.exp(scores - top)
        probs = (expd / (lax.optimization_barrier(jnp.sum(expd, axis=-1, keepdims=True)) + jnp.exp(sink_table - top))).astype(jnp.bfloat16)
        mixed = jnp.einsum('hgqk,khd->qhgd', probs.astype(jnp.float32), values)
        return mixed.reshape(WINDOW, HEADS * HEAD).astype(jnp.bfloat16)
    attended = lax.map(attend_block, jnp.arange(block_count, dtype=jnp.int32)).reshape(TOKENS, HEADS * HEAD)
    mixer_sum = jnp.dot(attended, w_out, preferred_element_type=jnp.float32)
    middle = resid.astype(jnp.float32) + mixer_sum
    normed = (middle * lax.rsqrt(lax.optimization_barrier(jnp.mean(middle * middle, axis=-1, keepdims=True)) + norm_eps) * norm_gain).astype(jnp.bfloat16)
    ffn_width = FF // N_TP

    def ffn_block(block_rows):
        gate = jnp.dot(block_rows, w_gate, preferred_element_type=jnp.float32)
        up_part = jnp.dot(block_rows, w_up, preferred_element_type=jnp.float32)
        hidden = (jax.nn.silu(gate) * up_part).astype(jnp.bfloat16)
        total = jnp.zeros((block_rows.shape[0], D), jnp.float32)
        for group in range(N_TP):
            lower = group * ffn_width
            partial_down = jnp.dot(hidden[:, lower:lower + ffn_width], w_down[lower:lower + ffn_width], preferred_element_type=jnp.float32).astype(jnp.bfloat16)
            total = total + lax.optimization_barrier(partial_down).astype(jnp.float32)
        return total
    ffn_sum = lax.map(ffn_block, normed.reshape(N_SP, TOK_DEV, D)).reshape(TOKENS, D)
    return (middle + ffn_sum).astype(jnp.bfloat16)
```

```python
import functools

import jax
import jax.numpy as jnp
from jax import lax
from jax.experimental import pallas as pl
from jax.experimental.pallas import tpu as pltpu
from jax.sharding import PartitionSpec as P

HEAD = 64
WINDOW = 128

norm_eps = 1e-06
masked = -1e30


def swap(block, sp_mask=0, tp_mask=0):
    n_sp, n_tp = lax.axis_size("sp"), lax.axis_size("tp")
    if sp_mask and tp_mask:
        pairs = [
            (s * n_tp + t, (s ^ sp_mask) * n_tp + (t ^ tp_mask))
            for s in range(n_sp)
            for t in range(n_tp)
        ]
        return lax.ppermute(block, ("sp", "tp"), pairs)
    if sp_mask:
        return lax.ppermute(block, "sp", [(s, s ^ sp_mask) for s in range(n_sp)])
    if tp_mask:
        return lax.ppermute(block, "tp", [(t, t ^ tp_mask) for t in range(n_tp)])
    return block


def edges(block, width):
    count = lax.axis_size("sp")
    forward = [(i, i + 1) for i in range(count - 1)]
    backward = [(b, a) for a, b in forward]
    low = lax.ppermute(block[block.shape[0] - width :], "sp", forward)
    high = lax.ppermute(block[:width], "sp", backward)
    return low, high


def band_view(extended, block_count):
    shaped = extended.reshape((block_count + 2, WINDOW) + extended.shape[1:])
    return jnp.concatenate([shaped[:-2], shaped[1:-1], shaped[2:]], axis=1)


def attention(q_proj, k_proj, v_proj, doc_ids, sinks):
    tok_rows = q_proj.shape[0]
    kv_local = k_proj.shape[1] // HEAD
    groups = q_proj.shape[1] // HEAD // kv_local
    block_count = tok_rows // WINDOW
    kv_cols = k_proj.shape[1]
    kv = jnp.concatenate([k_proj, v_proj], axis=1)
    kv_low, kv_high = edges(kv, WINDOW)
    doc_low, doc_high = edges(doc_ids, WINDOW)
    kv_ext = jnp.concatenate([kv_low, kv, kv_high], axis=0)
    docs_ext = jnp.concatenate([doc_low, doc_ids, doc_high], axis=0)
    positions = (
        lax.axis_index("sp") * tok_rows
        - WINDOW
        + jnp.arange(tok_rows + 2 * WINDOW, dtype=jnp.int32)
    )
    inside = (positions >= 0) & (positions < tok_rows * lax.axis_size("sp"))
    docs_ext = jnp.where(inside, docs_ext, -1)
    keys_ext, values_ext = kv_ext[:, :kv_cols], kv_ext[:, kv_cols:]
    key_band = band_view(keys_ext.reshape(tok_rows + 2 * WINDOW, kv_local, HEAD), block_count)
    value_band = band_view(values_ext.reshape(tok_rows + 2 * WINDOW, kv_local, HEAD), block_count)
    doc_band = band_view(docs_ext, block_count)
    queries = q_proj.reshape(block_count, WINDOW, kv_local, groups, HEAD)
    scores = jnp.einsum(
        "bqhgd,bkhd->bhgqk", queries, key_band, preferred_element_type=jnp.float32
    ) * HEAD ** (-0.5)
    offsets = jnp.arange(3 * WINDOW, dtype=jnp.int32) - WINDOW
    near = jnp.abs(jnp.arange(WINDOW, dtype=jnp.int32)[:, None] - offsets[None, :]) <= WINDOW
    query_docs = doc_ids.reshape(block_count, WINDOW)
    valid = near[None] & (query_docs[:, :, None] == doc_band[:, None, :])
    scores = jnp.where(valid[:, None, None], scores, masked)
    sink_table = sinks.reshape(kv_local, groups)[None, :, :, None, None]
    top = jnp.maximum(jnp.max(scores, axis=-1, keepdims=True), sink_table)
    expd = jnp.exp(scores - top)
    probs = (expd / (jnp.sum(expd, axis=-1, keepdims=True) + jnp.exp(sink_table - top))).astype(
        jnp.bfloat16
    )
    attended = jnp.einsum(
        "bhgqk,bkhd->bqhgd", probs, value_band, preferred_element_type=jnp.float32
    )
    return attended.astype(jnp.bfloat16).reshape(tok_rows, kv_local * groups * HEAD)


VMEM = pl.BlockSpec(memory_space=pltpu.VMEM)
ANY = pl.BlockSpec(memory_space=pl.ANY)


def project_kernel(count, resid_ref, gain_ref, *refs):
    heads, weights, (middle_ref, normed_ref) = refs[:count], refs[count : 2 * count], refs[2 * count :]
    width = middle_ref.shape[1]
    tile = min(512, width)
    squares = jnp.zeros((middle_ref.shape[0], 1), jnp.float32)
    for lower in range(0, width, tile):
        cols = pl.ds(lower, tile)
        total = resid_ref[:, cols].astype(jnp.float32)
        for head, weight in zip(heads, weights):
            total += jnp.dot(head[...], weight[:, cols], preferred_element_type=jnp.float32)
        middle_ref[:, cols] = total
        squares += jnp.sum(total * total, axis=-1, keepdims=True)
    factor = lax.rsqrt(squares / width + norm_eps)
    for lower in range(0, width, tile):
        cols = pl.ds(lower, tile)
        normed_ref[:, cols] = (middle_ref[:, cols] * factor * gain_ref[:, cols]).astype(jnp.bfloat16)


def project(resid, gain, heads, weights):
    rows, width = resid.shape
    count = len(heads)
    return pl.pallas_call(
        functools.partial(project_kernel, count),
        out_shape=(
            jax.ShapeDtypeStruct((rows, width), jnp.float32),
            jax.ShapeDtypeStruct((rows, width), jnp.bfloat16),
        ),
        in_specs=[VMEM] * (2 + 2 * count),
        out_specs=(VMEM, VMEM),
        cost_estimate=pl.CostEstimate(
            flops=2 * rows * width * count * heads[0].shape[1], bytes_accessed=6 << 20, transcendentals=0
        ),
    )(resid, gain, *heads, *weights)


def hidden_kernel(n_rows, n_parts, starts_ref, *refs):
    row_refs, part_refs = refs[:n_rows], refs[n_rows : n_rows + n_parts]
    hidden_ref, rows, weight, row_sems, part_sems = refs[n_rows + n_parts :]
    copies = []
    height = row_refs[0].shape[0]
    for i, ref in enumerate(row_refs):
        copies.append(pltpu.make_async_copy(ref, rows.at[pl.ds(i * height, height)], row_sems.at[i]))
    for i, ref in enumerate(part_refs):
        start = pl.multiple_of(starts_ref[i], ref.shape[0])
        copies.append(pltpu.make_async_copy(ref, weight.at[pl.ds(start, ref.shape[0])], part_sems.at[i]))
    for copy in copies:
        copy.start()
    for copy in copies:
        copy.wait()
    half = hidden_ref.shape[1]
    tile = min(256, rows.shape[0])

    def step(i, carry):
        part = pl.ds(pl.multiple_of(i * tile, tile), tile)
        both = jnp.dot(rows[part, :], weight[...], preferred_element_type=jnp.float32)
        gate, up = both[:, :half], both[:, half:]
        hidden_ref[part, :] = (gate / (1.0 + jnp.exp(-gate)) * up).astype(jnp.bfloat16)
        return carry

    lax.fori_loop(0, rows.shape[0] // tile, step, 0)


def hidden_units(starts, row_blocks, parts):
    rows = sum(block.shape[0] for block in row_blocks)
    depth, width = row_blocks[0].shape[1], parts[0].shape[1]
    return pl.pallas_call(
        functools.partial(hidden_kernel, len(row_blocks), len(parts)),
        out_shape=jax.ShapeDtypeStruct((rows, width // 2), jnp.bfloat16),
        in_specs=[pl.BlockSpec(memory_space=pltpu.SMEM)] + [ANY] * (len(row_blocks) + len(parts)),
        out_specs=VMEM,
        scratch_shapes=[
            pltpu.VMEM((rows, depth), jnp.bfloat16),
            pltpu.VMEM((depth, width), jnp.bfloat16),
            pltpu.SemaphoreType.DMA((len(row_blocks),)),
            pltpu.SemaphoreType.DMA((len(parts),)),
        ],
        cost_estimate=pl.CostEstimate(
            flops=2 * rows * width * depth, bytes_accessed=11 << 20, transcendentals=rows * width // 2
        ),
        compiler_params=pltpu.CompilerParams(vmem_limit_bytes=40 << 20),
    )(starts, *row_blocks, *parts)


def down_kernel(n_parts, starts_ref, hidden_ref, *refs):
    part_refs, (keep_ref, send_ref, weight, sems) = refs[:n_parts], refs[n_parts:]
    copies = []
    for i, ref in enumerate(part_refs):
        start = pl.multiple_of(starts_ref[i], ref.shape[1]) if n_parts > 1 else 0
        copies.append(pltpu.make_async_copy(ref, weight.at[:, pl.ds(start, ref.shape[1])], sems.at[i]))
    for copy in copies:
        copy.start()
    for copy in copies:
        copy.wait()
    keep = keep_ref.shape[0]
    tile = min(256, keep)
    for target, base in ((send_ref, keep), (keep_ref, 0)):
        for lower in range(0, keep, tile):
            target[pl.ds(lower, tile), :] = jnp.dot(
                hidden_ref[pl.ds(base + lower, tile), :], weight[...], preferred_element_type=jnp.float32
            ).astype(jnp.bfloat16)


def down_rows(starts, hidden, parts):
    rows, depth = hidden.shape
    width = sum(part.shape[1] for part in parts)
    shape = jax.ShapeDtypeStruct((rows // 2, width), jnp.bfloat16)
    return pl.pallas_call(
        functools.partial(down_kernel, len(parts)),
        out_shape=(shape, shape),
        in_specs=[pl.BlockSpec(memory_space=pltpu.SMEM), VMEM] + [ANY] * len(parts),
        out_specs=(VMEM, VMEM),
        scratch_shapes=[
            pltpu.VMEM((depth, width), jnp.bfloat16),
            pltpu.SemaphoreType.DMA((len(parts),)),
        ],
        cost_estimate=pl.CostEstimate(
            flops=2 * rows * width * depth, bytes_accessed=4 << 20, transcendentals=0
        ),
        compiler_params=pltpu.CompilerParams(vmem_limit_bytes=24 << 20),
    )(starts, hidden, *parts)


def lay_out(parts, starts, axis):
    total = sum(part.shape[axis] for part in parts)
    shape = list(parts[0].shape)
    shape[axis] = total
    whole = jnp.zeros(shape, parts[0].dtype)
    for part, start in zip(parts, starts):
        whole = lax.dynamic_update_slice_in_dim(whole, part, start, axis)
    return whole


def shards(q_proj, k_proj, v_proj, doc_ids, sinks, resid, w_out, norm_gain, w_gate, w_up, w_down):
    n_sp, n_tp = lax.axis_size("sp"), lax.axis_size("tp")
    n_y = 1 << ((n_sp.bit_length() - 1) // 2)
    n_z = n_sp // n_y
    sp, tp = lax.axis_index("sp"), lax.axis_index("tp")
    z = sp // n_y
    own_half = z % 2
    half = w_gate.shape[1] // 2
    depth = w_gate.shape[0]
    piece = w_down.shape[1]

    lower = jnp.concatenate([w_gate[:, :half], w_up[:, :half]], axis=1)
    upper = jnp.concatenate([w_gate[:, half:], w_up[:, half:]], axis=1)
    first = own_half == 0
    gu_half = (jnp.where(first, lower, upper), jnp.where(first, upper, lower))
    down_half = (
        jnp.where(first, w_down[:half], w_down[half:]),
        jnp.where(first, w_down[half:], w_down[:half]),
    )

    attended = attention(q_proj, k_proj, v_proj, doc_ids, sinks)

    gu, down = {}, {}
    for dz in range(n_z):
        gu[dz, 0] = swap(gu_half[dz % 2], dz * n_y)
        for dy in range(1, n_y):
            gu[dz, dy] = swap(gu[dz, 0], dy)
    for dz in range(n_z):
        down[dz, 0] = swap(down_half[dz % 2], dz * n_y)
        for dy in range(1, n_y):
            down[dz, dy] = swap(down[dz, 0], dy)

    out_blocks = [w_out]
    for t in range(2, n_tp, 2):
        out_blocks.append(swap(w_out, 0, t))
    out_blocks = {2 * i + c: swap(b, 0, c) for i, b in enumerate(out_blocks) for c in (0, 1)}
    own_rows = tok_rows = q_proj.shape[0] // n_tp
    heads = [
        swap(lax.dynamic_slice_in_dim(attended, (tp ^ t) * own_rows, own_rows, 0), 0, t)
        for t in range(n_tp)
    ]
    middle, normed = project(
        resid, norm_gain[None, :], heads, [out_blocks[t] for t in range(n_tp)]
    )

    rows = {(0, 0): normed, (1, 0): swap(normed, n_y)}
    for t in range(2, n_tp, 2):
        rows[0, t] = swap(normed, 0, t)
        rows[1, t] = swap(rows[1, 0], 0, t)
    for (a, t), block in list(rows.items()):
        rows[a, t + 1] = swap(block, 0, 1)
    order = [(a, t + c) for c in (0, 1) for a in (0, 1) for t in range(0, n_tp, 2)]

    keys = list(gu)
    starts = [(sp ^ (dz * n_y + dy)) * depth for dz, dy in keys]
    parts = [gu[key] for key in keys]
    hidden = hidden_units(jnp.stack(starts).astype(jnp.int32), [rows[key] for key in order], parts)

    out = jnp.zeros(resid.shape, jnp.bfloat16)
    span = 2 * n_y * piece
    for pair in range(n_z // 2):
        chunk_keys = [(2 * pair + b, dy) for b in (0, 1) for dy in range(n_y)]
        starts = [((sp ^ (dz * n_y + dy)) % (2 * n_y)) * piece for dz, dy in chunk_keys]
        parts = [down[key] for key in chunk_keys]
        if piece % 128:
            parts, starts = [lay_out(parts, starts, 1)], [sp * 0]
        keep, send = down_rows(jnp.stack(starts).astype(jnp.int32), hidden, parts)
        total = (keep.astype(jnp.float32) + swap(send, 0, 1).astype(jnp.float32)).astype(jnp.bfloat16)
        base = (z // 2 ^ pair) * span
        result = lax.dynamic_slice_in_dim(middle, base, span, 1)
        for i, (a, t) in enumerate(order[: len(order) // 2]):
            result = result + swap(total[i * own_rows : (i + 1) * own_rows], a * n_y, t).astype(jnp.float32)
        out = lax.dynamic_update_slice_in_dim(out, result.astype(jnp.bfloat16), base, 1)
    return out


def solution(mesh):
    placed = (
        P("sp", "tp"),
        P("sp", "tp"),
        P("sp", "tp"),
        P("sp"),
        P("tp"),
        P(("sp", "tp"), None),
        P("tp", None),
        P(),
        P("sp", "tp"),
        P("sp", "tp"),
        P("tp", "sp"),
    )
    return jax.shard_map(
        shards, mesh=mesh, in_specs=placed, out_specs=P(("sp", "tp"), None), check_vma=False
    )
```

```python
import functools

import jax
import jax.numpy as jnp
from jax import lax
from jax.experimental import pallas as pl
from jax.experimental.pallas import tpu as pltpu
from jax.sharding import PartitionSpec as P


HEAD = 64
WINDOW = 128

norm_eps = 1e-06
masked = -1e30


def swap(block, sp_mask=0, tp_mask=0):
    n_sp, n_tp = lax.axis_size("sp"), lax.axis_size("tp")
    if sp_mask and tp_mask:
        axis = ("sp", "tp")
        pairs = [
            (s * n_tp + t, (s ^ sp_mask) * n_tp + (t ^ tp_mask))
            for s in range(n_sp)
            for t in range(n_tp)
        ]
    elif sp_mask:
        axis, pairs = "sp", [(s, s ^ sp_mask) for s in range(n_sp)]
    elif tp_mask:
        axis, pairs = "tp", [(t, t ^ tp_mask) for t in range(n_tp)]
    else:
        return block
    return lax.ppermute(block, axis, pairs)


def edges(block, width):
    count = lax.axis_size("sp")
    forward = [(i, i + 1) for i in range(count - 1)]
    backward = [(b, a) for a, b in forward]
    low = lax.ppermute(block[block.shape[0] - width :], "sp", forward)
    high = lax.ppermute(block[:width], "sp", backward)
    return low, high


def attention_kernel(sinks_ref, docs_ref, q_ref, k_ref, v_ref, low_ref, high_ref, out_ref):
    kv_cols = k_ref.shape[1]
    kv_heads = kv_cols // HEAD
    groups = q_ref.shape[1] // kv_cols
    count = q_ref.shape[0] // WINDOW
    span = 3 * WINDOW
    shape = (WINDOW, span)
    offset = lax.broadcasted_iota(jnp.int32, shape, 1) - lax.broadcasted_iota(jnp.int32, shape, 0)
    near = (offset >= 0) & (offset <= 2 * WINDOW)

    def band(own_ref, column, block):
        pieces = []
        for i in range(block - 1, block + 2):
            if i < 0:
                pieces.append(low_ref[:, column : column + kv_cols])
            elif i == count:
                pieces.append(high_ref[:, column : column + kv_cols])
            else:
                pieces.append(own_ref[i * WINDOW : (i + 1) * WINDOW, :])
        return jnp.concatenate(pieces, axis=0)

    for block in range(count):
        rows = slice(block * WINDOW, (block + 1) * WINDOW)
        own_docs = docs_ref[:, (block + 1) * WINDOW : (block + 2) * WINDOW]
        query_docs = jnp.broadcast_to(own_docs, (WINDOW, WINDOW)).T
        band_docs = docs_ref[:, block * WINDOW : block * WINDOW + span]
        valid = near & (jnp.concatenate([query_docs] * 3, axis=1) == band_docs)
        keys, values = band(k_ref, 0, block), band(v_ref, kv_cols, block)
        outs = []
        for head in range(kv_heads):
            cols = slice(head * HEAD, (head + 1) * HEAD)
            for group in range(groups):
                index = head * groups + group
                query = q_ref[rows, index * HEAD : (index + 1) * HEAD]
                scores = lax.dot_general(
                    query, keys[:, cols], (((1,), (1,)), ((), ())), preferred_element_type=jnp.float32
                ) * HEAD ** (-0.5)
                scores = jnp.where(valid, scores, masked)
                sink = sinks_ref[index]
                top = jnp.maximum(jnp.max(scores, axis=-1, keepdims=True), sink)
                expd = jnp.exp(scores - top)
                total = jnp.sum(expd, axis=-1, keepdims=True) + jnp.exp(sink - top)
                probs = (expd * (1.0 / total)).astype(jnp.bfloat16)
                outs.append(jnp.dot(probs, values[:, cols], preferred_element_type=jnp.float32))
        out_ref[rows, :] = jnp.concatenate(outs, axis=1).astype(jnp.bfloat16)


def attention(q_proj, k_proj, v_proj, doc_ids, sinks):
    tok_rows = q_proj.shape[0]
    kv = jnp.concatenate([k_proj, v_proj], axis=1)
    kv_low, kv_high = edges(kv, WINDOW)
    doc_low, doc_high = edges(doc_ids, WINDOW)
    docs = jnp.concatenate([doc_low, doc_ids, doc_high], axis=0)
    positions = (
        lax.axis_index("sp") * tok_rows
        - WINDOW
        + jnp.arange(tok_rows + 2 * WINDOW, dtype=jnp.int32)
    )
    inside = (positions >= 0) & (positions < tok_rows * lax.axis_size("sp"))
    docs = jnp.where(inside, docs, -1)[None, :]
    return pl.pallas_call(
        attention_kernel,
        out_shape=jax.ShapeDtypeStruct(q_proj.shape, jnp.bfloat16),
        in_specs=[SMEM] + [VMEM] * 6,
        out_specs=VMEM,
        cost_estimate=pl.CostEstimate(
            flops=12 * tok_rows * WINDOW * q_proj.shape[1],
            bytes_accessed=1 << 20,
            transcendentals=0,
        ),
    )(sinks, docs, q_proj, k_proj, v_proj, kv_low, kv_high)


SMEM = pl.BlockSpec(memory_space=pltpu.SMEM)
VMEM = pl.BlockSpec(memory_space=pltpu.VMEM)
ANY = pl.BlockSpec(memory_space=pl.ANY)


def project_kernel(count, resid_ref, gain_ref, *refs):
    heads, weights, (middle_ref, normed_ref) = refs[:count], refs[count : 2 * count], refs[2 * count :]
    width = middle_ref.shape[1]
    tile = min(512, width)
    squares = jnp.zeros((middle_ref.shape[0], 1), jnp.float32)
    for lower in range(0, width, tile):
        cols = pl.ds(lower, tile)
        total = resid_ref[:, cols].astype(jnp.float32)
        for head, weight in zip(heads, weights):
            total += jnp.dot(head[...], weight[:, cols], preferred_element_type=jnp.float32)
        middle_ref[:, cols] = total
        squares += jnp.sum(total * total, axis=-1, keepdims=True)
    factor = lax.rsqrt(squares / width + norm_eps)
    for lower in range(0, width, tile):
        cols = pl.ds(lower, tile)
        normed_ref[:, cols] = (middle_ref[:, cols] * factor * gain_ref[:, cols]).astype(jnp.bfloat16)


def project(resid, gain, heads, weights):
    rows, width = resid.shape
    count = len(heads)
    return pl.pallas_call(
        functools.partial(project_kernel, count),
        out_shape=(
            jax.ShapeDtypeStruct((rows, width), jnp.float32),
            jax.ShapeDtypeStruct((rows, width), jnp.bfloat16),
        ),
        in_specs=[VMEM] * (2 + 2 * count),
        out_specs=(VMEM, VMEM),
        cost_estimate=pl.CostEstimate(
            flops=2 * rows * width * count * heads[0].shape[1], bytes_accessed=6 << 20, transcendentals=0
        ),
    )(resid, gain, *heads, *weights)


def hidden_kernel(n_rows, n_parts, starts_ref, *refs):
    row_refs, part_refs = refs[:n_rows], refs[n_rows : n_rows + n_parts]
    hidden_ref, rows, weight, row_sems, part_sems = refs[n_rows + n_parts :]
    copies = []
    height = row_refs[0].shape[0]
    for i, ref in enumerate(row_refs):
        copies.append(pltpu.make_async_copy(ref, rows.at[pl.ds(i * height, height)], row_sems.at[i]))
    for i, ref in enumerate(part_refs):
        start = pl.multiple_of(starts_ref[i], ref.shape[0])
        copies.append(pltpu.make_async_copy(ref, weight.at[pl.ds(start, ref.shape[0])], part_sems.at[i]))
    for copy in copies[n_rows:] + copies[:n_rows]:
        copy.start()
    for copy in copies[n_rows:]:
        copy.wait()
    half = hidden_ref.shape[1]
    tile = min(256, rows.shape[0])
    for lower in range(0, rows.shape[0], tile):
        for i in range(lower // height, (lower + tile) // height):
            copies[i].wait()
        both = jnp.dot(rows[pl.ds(lower, tile), :], weight[...], preferred_element_type=jnp.float32)
        gate, up = both[:, :half], both[:, half:]
        hidden_ref[pl.ds(lower, tile), :] = (gate / (1.0 + jnp.exp(-gate)) * up).astype(jnp.bfloat16)


def hidden_units(starts, row_blocks, parts):
    rows = sum(block.shape[0] for block in row_blocks)
    depth, width = row_blocks[0].shape[1], parts[0].shape[1]
    return pl.pallas_call(
        functools.partial(hidden_kernel, len(row_blocks), len(parts)),
        out_shape=jax.ShapeDtypeStruct((rows, width // 2), jnp.bfloat16),
        in_specs=[SMEM] + [ANY] * (len(row_blocks) + len(parts)),
        out_specs=VMEM,
        scratch_shapes=[
            pltpu.VMEM((rows, depth), jnp.bfloat16),
            pltpu.VMEM((depth, width), jnp.bfloat16),
            pltpu.SemaphoreType.DMA((len(row_blocks),)),
            pltpu.SemaphoreType.DMA((len(parts),)),
        ],
        cost_estimate=pl.CostEstimate(
            flops=2 * rows * width * depth, bytes_accessed=11 << 20, transcendentals=rows * width // 2
        ),
        compiler_params=pltpu.CompilerParams(vmem_limit_bytes=40 << 20),
    )(starts, *row_blocks, *parts)


def down_kernel(n_parts, starts_ref, hidden_ref, *refs):
    part_refs, (keep_ref, send_ref, weight, sems) = refs[:n_parts], refs[n_parts:]
    copies = []
    for i, ref in enumerate(part_refs):
        start = pl.multiple_of(starts_ref[i], ref.shape[1]) if n_parts > 1 else 0
        copies.append(pltpu.make_async_copy(ref, weight.at[:, pl.ds(start, ref.shape[1])], sems.at[i]))
    for copy in copies:
        copy.start()
    for copy in copies:
        copy.wait()
    keep = keep_ref.shape[0]
    tile = min(256, keep)
    for target, base in ((send_ref, keep), (keep_ref, 0)):
        for lower in range(0, keep, tile):
            target[pl.ds(lower, tile), :] = jnp.dot(
                hidden_ref[pl.ds(base + lower, tile), :], weight[...], preferred_element_type=jnp.float32
            ).astype(jnp.bfloat16)


def down_rows(starts, hidden, parts):
    rows, depth = hidden.shape
    width = sum(part.shape[1] for part in parts)
    shape = jax.ShapeDtypeStruct((rows // 2, width), jnp.bfloat16)
    return pl.pallas_call(
        functools.partial(down_kernel, len(parts)),
        out_shape=(shape, shape),
        in_specs=[SMEM, VMEM] + [ANY] * len(parts),
        out_specs=(VMEM, VMEM),
        scratch_shapes=[
            pltpu.VMEM((depth, width), jnp.bfloat16),
            pltpu.SemaphoreType.DMA((len(parts),)),
        ],
        cost_estimate=pl.CostEstimate(
            flops=2 * rows * width * depth, bytes_accessed=4 << 20, transcendentals=0
        ),
        compiler_params=pltpu.CompilerParams(vmem_limit_bytes=24 << 20),
    )(starts, hidden, *parts)


def finish_kernel(plan, per_chunk, bases_ref, middle_ref, *refs):
    out_ref = refs[-1]
    for chunk, (strips, pitch, shift) in enumerate(plan):
        totals = refs[chunk * per_chunk : (chunk + 1) * per_chunk]
        width = totals[0].shape[1] // strips
        for strip in range(strips):
            start = bases_ref[chunk] + (strip * pitch + shift)
            cols = pl.ds(pl.multiple_of(start, width), width)
            total = middle_ref[:, cols]
            for ref in totals:
                total += ref[:, strip * width : (strip + 1) * width].astype(jnp.float32)
            out_ref[:, cols] = total.astype(jnp.bfloat16)


def finish(plan, bases, middle, chunks):
    return pl.pallas_call(
        functools.partial(finish_kernel, plan, len(chunks[0])),
        out_shape=jax.ShapeDtypeStruct(middle.shape, jnp.bfloat16),
        in_specs=[SMEM] + [VMEM] * (1 + len(chunks) * len(chunks[0])),
        out_specs=VMEM,
        cost_estimate=pl.CostEstimate(
            flops=8 * middle.size, bytes_accessed=8 * middle.size, transcendentals=0
        ),
    )(bases, middle, *[block for chunk in chunks for block in chunk])


def lay_out(parts, starts, axis):
    total = sum(part.shape[axis] for part in parts)
    shape = list(parts[0].shape)
    shape[axis] = total
    whole = jnp.zeros(shape, parts[0].dtype)
    for part, start in zip(parts, starts):
        whole = lax.dynamic_update_slice_in_dim(whole, part, start, axis)
    return whole


def y_count(n_sp):
    return 1 << ((n_sp.bit_length() - 1) // 2)


def shards(q_proj, k_proj, v_proj, doc_ids, sinks, resid, w_out, norm_gain, w_gate, w_up, w_down):
    n_sp, n_tp = lax.axis_size("sp"), lax.axis_size("tp")
    n_y = y_count(n_sp)
    n_z = n_sp // n_y
    sp, tp = lax.axis_index("sp"), lax.axis_index("tp")
    z = sp // n_y
    half = w_gate.shape[1] // 2
    depth = w_gate.shape[0]
    piece = w_down.shape[1]

    lower = jnp.concatenate([w_gate[:, :half], w_up[:, :half]], axis=1)
    upper = jnp.concatenate([w_gate[:, half:], w_up[:, half:]], axis=1)
    first = z % 2 == 0
    gu_half = (jnp.where(first, lower, upper), jnp.where(first, upper, lower))
    down_half = (
        jnp.where(first, w_down[:half], w_down[half:]),
        jnp.where(first, w_down[half:], w_down[:half]),
    )

    gu_parts, gu_starts = [], []
    for dz in range(n_z):
        cuts = 1 if dz < 2 else 2
        height = depth // cuts
        for cut in range(cuts):
            held = swap(gu_half[dz % 2][cut * height : (cut + 1) * height], dz * n_y)
            for dy in range(n_y):
                gu_parts.append(swap(held, dy))
                gu_starts.append((sp ^ (dz * n_y + dy)) * depth + cut * height)
    down, cuts_of = {}, {}
    for dz in range(n_z):
        cuts = cuts_of[dz // 2] = 2 if dz >= 2 and piece % 256 == 0 else 1
        width = piece // cuts
        for cut in range(cuts):
            held = swap(down_half[dz % 2][:, cut * width : (cut + 1) * width], dz * n_y)
            for dy in range(n_y):
                down[dz, cut, dy] = swap(held, dy)

    attended = attention(q_proj, k_proj, v_proj, doc_ids, sinks)

    out_blocks = {}
    for t in range(0, n_tp, 2):
        out_blocks[t] = swap(w_out, 0, t)
        out_blocks[t + 1] = swap(out_blocks[t], 0, 1)
    own_rows = q_proj.shape[0] // n_tp
    heads = [swap(lax.dynamic_slice_in_dim(attended, (tp ^ t) * own_rows, own_rows, 0), 0, t) for t in range(n_tp)]
    middle, normed = project(
        resid, norm_gain[None, :], heads, [out_blocks[t] for t in range(n_tp)]
    )

    rows = {(0, 0): normed, (1, 0): swap(normed, n_y)}
    for t in range(2, n_tp, 2):
        for a in (0, 1):
            rows[a, t] = swap(rows[a, 0], 0, t)
    for (a, t), block in list(rows.items()):
        rows[a, t + 1] = swap(block, 0, 1)
    order = [(a, t + c) for c in (0, 1) for a in (0, 1) for t in range(0, n_tp, 2)]

    hidden = hidden_units(
        jnp.stack(gu_starts).astype(jnp.int32), [rows[key] for key in order], gu_parts
    )

    plan, bases, chunks = [], [], []
    span = 2 * n_y * piece
    for pair, cuts in cuts_of.items():
        width = piece // cuts
        for cut in range(cuts):
            keys = [(2 * pair + b, dy) for b in (0, 1) for dy in range(n_y)]
            starts = [((sp ^ (dz * n_y + dy)) % (2 * n_y)) * width for dz, dy in keys]
            parts = [down[dz, cut, dy] for dz, dy in keys]
            if width % 128:
                parts, starts = [lay_out(parts, starts, 1)], [sp * 0]
            keep, send = down_rows(jnp.stack(starts).astype(jnp.int32), hidden, parts)
            other = swap(send, 0, 1)
            total = (keep.astype(jnp.float32) + other.astype(jnp.float32)).astype(jnp.bfloat16)
            plan.append((1, span, 0) if cuts == 1 else (2 * n_y, piece, cut * width))
            bases.append((z // 2 ^ pair) * span)
            chunks.append(
                [
                    swap(total[i * own_rows : (i + 1) * own_rows], a * n_y, t)
                    for i, (a, t) in enumerate(order[: len(order) // 2])
                ]
            )
    return finish(tuple(plan), jnp.stack(bases).astype(jnp.int32), middle, chunks)


def solution(mesh):
    placed = (
        P("sp", "tp"),
        P("sp", "tp"),
        P("sp", "tp"),
        P("sp"),
        P("tp"),
        P(("sp", "tp"), None),
        P("tp", None),
        P(),
        P("sp", "tp"),
        P("sp", "tp"),
        P("tp", "sp"),
    )

    return jax.shard_map(shards, mesh=mesh, in_specs=placed, out_specs=P(("sp", "tp"), None), check_vma=False)
```

```python
import functools

import jax
import jax.numpy as jnp
from jax import lax
from jax.experimental import pallas as pl
from jax.experimental.pallas import tpu as pltpu
from jax.sharding import PartitionSpec as P


HEAD = 64
WINDOW = 128

norm_eps = 1e-06
masked = -1e30


def swap(block, sp_mask=0, tp_mask=0):
    n_sp, n_tp = lax.axis_size("sp"), lax.axis_size("tp")
    if sp_mask and tp_mask:
        axis = ("sp", "tp")
        pairs = [
            (s * n_tp + t, (s ^ sp_mask) * n_tp + (t ^ tp_mask))
            for s in range(n_sp)
            for t in range(n_tp)
        ]
    elif sp_mask:
        axis, pairs = "sp", [(s, s ^ sp_mask) for s in range(n_sp)]
    elif tp_mask:
        axis, pairs = "tp", [(t, t ^ tp_mask) for t in range(n_tp)]
    else:
        return block
    return lax.ppermute(block, axis, pairs)


def attention_kernel(n_out, info_ref, sinks_ref, docs_ref, q_ref, k_ref, v_ref, first_ref, second_ref, *refs):
    out_refs, attended = refs[:n_out], refs[n_out]
    kv_cols = k_ref.shape[1]
    kv_heads = kv_cols // HEAD
    groups = q_ref.shape[1] // kv_cols
    count = q_ref.shape[0] // WINDOW
    span = 3 * WINDOW
    shape = (WINDOW, span)
    even = info_ref[1] == 0
    offset = lax.broadcasted_iota(jnp.int32, shape, 1) - lax.broadcasted_iota(jnp.int32, shape, 0)
    near = (offset >= 0) & (offset <= 2 * WINDOW)
    ones = jnp.ones((span, HEAD), jnp.bfloat16)

    def band(own_ref, column, block):
        cols = slice(column, column + kv_cols)
        pieces = []
        for i in range(block - 1, block + 2):
            if 0 <= i < count:
                pieces.append(own_ref[i * WINDOW : (i + 1) * WINDOW, :])
            elif i < 0:
                pieces.append(jnp.where(even, second_ref[:, cols], first_ref[:, cols]))
            else:
                pieces.append(jnp.where(even, first_ref[:, cols], second_ref[:, cols]))
        return jnp.concatenate(pieces, axis=0)

    for block in range(count):
        rows = slice(block * WINDOW, (block + 1) * WINDOW)
        own_docs = docs_ref[:, (block + 1) * WINDOW : (block + 2) * WINDOW]
        query_docs = jnp.broadcast_to(own_docs, (WINDOW, WINDOW)).T
        band_docs = docs_ref[:, block * WINDOW : block * WINDOW + span]
        valid = near & (jnp.concatenate([query_docs] * 3, axis=1) == band_docs)
        keys, values = band(k_ref, 0, block), band(v_ref, kv_cols, block)
        queries = q_ref[rows, :] * HEAD ** (-0.5)
        outs = []
        for head in range(kv_heads):
            cols = slice(head * HEAD, (head + 1) * HEAD)
            key = keys[:, cols]
            value = jnp.concatenate([values[:, cols], ones], axis=1)
            for group in range(groups):
                index = head * groups + group
                scores = lax.dot_general(
                    queries[:, index * HEAD : (index + 1) * HEAD],
                    key,
                    (((1,), (1,)), ((), ())),
                    preferred_element_type=jnp.float32,
                )
                scores = jnp.where(valid, scores, masked)
                sink = sinks_ref[index]
                top = jnp.maximum(jnp.max(scores, axis=-1, keepdims=True), sink)
                expd = jnp.exp(scores - top).astype(jnp.bfloat16)
                both = jnp.dot(expd, value, preferred_element_type=jnp.float32)
                outs.append(both[:, :HEAD] / (both[:, HEAD:] + jnp.exp(sink - top)))
        attended[rows, :] = jnp.concatenate(outs, axis=1).astype(jnp.bfloat16)
    height = out_refs[0].shape[0]
    for i, out_ref in enumerate(out_refs):
        out_ref[...] = attended[pl.ds(pl.multiple_of((info_ref[0] ^ i) * height, height), height), :]


def attention(q_proj, k_proj, v_proj, doc_ids, sinks):
    tok_rows = q_proj.shape[0]
    n_tp, sp = lax.axis_size("tp"), lax.axis_index("sp")
    kv = jnp.concatenate([k_proj, v_proj], axis=1)
    count = lax.axis_size("sp")
    even = sp % 2 == 0
    up = [(i, i + 1) for i in range(0, count - 1, 2)]
    down = [(i, i + 1) for i in range(1, count - 1, 2)]
    tail, head = slice(tok_rows - WINDOW, tok_rows), slice(0, WINDOW)

    def trade(pairs, block, up_first):
        sent = jnp.where(even == up_first, block[tail], block[head])
        return lax.ppermute(sent, "sp", pairs + [(b, a) for a, b in pairs])

    doc_first, doc_second = (trade(up, doc_ids, True), trade(down, doc_ids, False))
    kv_first, kv_second = trade(up, kv, True), trade(down, kv, False)
    docs = jnp.concatenate(
        [
            jnp.where(sp == 0, -1, jnp.where(even, doc_second, doc_first)),
            doc_ids,
            jnp.where(sp == count - 1, -1, jnp.where(even, doc_first, doc_second)),
        ]
    )[None, :]
    info = jnp.stack([lax.axis_index("tp"), sp % 2]).astype(jnp.int32)
    own = jax.ShapeDtypeStruct((tok_rows // n_tp, q_proj.shape[1]), jnp.bfloat16)
    return pl.pallas_call(
        functools.partial(attention_kernel, n_tp),
        out_shape=(own,) * n_tp,
        in_specs=[SMEM] * 2 + [VMEM] * 6,
        out_specs=(VMEM,) * n_tp,
        scratch_shapes=[pltpu.VMEM(q_proj.shape, jnp.bfloat16)],
        cost_estimate=pl.CostEstimate(
            flops=12 * tok_rows * WINDOW * q_proj.shape[1],
            bytes_accessed=1 << 20,
            transcendentals=0,
        ),
    )(info, sinks, docs, q_proj, k_proj, v_proj, kv_first, kv_second)


SMEM = pl.BlockSpec(memory_space=pltpu.SMEM)
VMEM = pl.BlockSpec(memory_space=pltpu.VMEM)
ANY = pl.BlockSpec(memory_space=pl.ANY)


def pack_kernel(half, far_cuts, info_ref, gate_ref, up_ref, *refs):
    whole, step = half // 128 * 128, gate_ref.shape[0] // far_cuts

    def fill(source, target_of):
        lower = source * half
        for start in range(0, whole, 128):
            for ref, shift in ((gate_ref, 0), (up_ref, 128)):
                target_of(2 * start + shift, ref[:, lower + start : lower + start + 128])
        if half > whole:
            rest = [ref[:, lower + whole : lower + half] for ref in (gate_ref, up_ref)]
            target_of(2 * whole, jnp.concatenate(rest, axis=1))

    for source in (0, 1):
        for parity in (0, 1):
            targets = refs[parity * (1 + far_cuts) : (parity + 1) * (1 + far_cuts)]

            def store(start, value):
                cols = slice(start, start + value.shape[1])
                targets[0][:, cols] = value
                for cut in range(far_cuts):
                    targets[1 + cut][:, cols] = value[cut * step : (cut + 1) * step]

            @pl.when(info_ref[0] == source ^ parity)
            def _():
                fill(source, store)


def pack_gate_up(info, w_gate, w_up, far_cuts):
    depth, width = w_gate.shape
    near = jax.ShapeDtypeStruct((depth, width), jnp.bfloat16)
    far = jax.ShapeDtypeStruct((depth // far_cuts, width), jnp.bfloat16)
    packed = pl.pallas_call(
        functools.partial(pack_kernel, width // 2, far_cuts),
        out_shape=((near,) + (far,) * far_cuts) * 2,
        in_specs=[SMEM, VMEM, VMEM],
        out_specs=(VMEM,) * (2 * (1 + far_cuts)),
        cost_estimate=pl.CostEstimate(flops=4 * depth * width, bytes_accessed=6 * w_gate.size, transcendentals=0),
    )(info, w_gate, w_up)
    return packed[: 1 + far_cuts], packed[1 + far_cuts :]


def split_kernel(far_cuts, info_ref, down_ref, *refs):
    half = refs[0].shape[0]
    for parity in (0, 1):
        targets = refs[parity * (1 + far_cuts) : (parity + 1) * (1 + far_cuts)]
        rows = pl.ds(pl.multiple_of((info_ref[0] ^ parity) * half, half), half)
        value = down_ref[rows, :]
        width = value.shape[1] // far_cuts
        targets[0][...] = value
        for cut in range(far_cuts):
            targets[1 + cut][...] = value[:, cut * width : (cut + 1) * width]


def split_down(info, w_down, far_cuts):
    depth, width = w_down.shape
    near = jax.ShapeDtypeStruct((depth // 2, width), jnp.bfloat16)
    far = jax.ShapeDtypeStruct((depth // 2, width // far_cuts), jnp.bfloat16)
    halves = pl.pallas_call(
        functools.partial(split_kernel, far_cuts),
        out_shape=((near,) + (far,) * far_cuts) * 2,
        in_specs=[SMEM, VMEM],
        out_specs=(VMEM,) * (2 * (1 + far_cuts)),
        cost_estimate=pl.CostEstimate(flops=depth * width, bytes_accessed=8 * depth * width, transcendentals=0),
    )(info, w_down)
    return halves[: 1 + far_cuts], halves[1 + far_cuts :]


def merge_kernel(keep_ref, other_ref, *out_refs):
    height = out_refs[0].shape[0]
    for i, out_ref in enumerate(out_refs):
        rows = pl.ds(i * height, height)
        total = keep_ref[rows, :].astype(jnp.float32) + other_ref[rows, :].astype(jnp.float32)
        out_ref[...] = total.astype(jnp.bfloat16)


def merge(keep, other, count):
    part = jax.ShapeDtypeStruct((keep.shape[0] // count, keep.shape[1]), jnp.bfloat16)
    return pl.pallas_call(
        merge_kernel,
        out_shape=(part,) * count,
        in_specs=[VMEM] * 2,
        out_specs=(VMEM,) * count,
        cost_estimate=pl.CostEstimate(flops=keep.size, bytes_accessed=6 * keep.size, transcendentals=0),
    )(keep, other)


def project_kernel(count, resid_ref, gain_ref, *refs):
    heads, weights, (middle_ref, normed_ref) = refs[:count], refs[count : 2 * count], refs[2 * count :]
    width = middle_ref.shape[1]
    tile = min(512, width)
    squares = jnp.zeros((middle_ref.shape[0], 1), jnp.float32)
    for lower in range(0, width, tile):
        cols = pl.ds(lower, tile)
        total = resid_ref[:, cols].astype(jnp.float32)
        for head, weight in zip(heads, weights):
            total += jnp.dot(head[...], weight[:, cols], preferred_element_type=jnp.float32)
        middle_ref[:, cols] = total
        squares += jnp.sum(total * total, axis=-1, keepdims=True)
    factor = lax.rsqrt(squares / width + norm_eps)
    for lower in range(0, width, tile):
        cols = pl.ds(lower, tile)
        normed_ref[:, cols] = (middle_ref[:, cols] * factor * gain_ref[:, cols]).astype(jnp.bfloat16)


def project(resid, gain, heads, weights):
    rows, width = resid.shape
    count = len(heads)
    return pl.pallas_call(
        functools.partial(project_kernel, count),
        out_shape=(
            jax.ShapeDtypeStruct((rows, width), jnp.float32),
            jax.ShapeDtypeStruct((rows, width), jnp.bfloat16),
        ),
        in_specs=[VMEM] * (2 + 2 * count),
        out_specs=(VMEM, VMEM),
        cost_estimate=pl.CostEstimate(
            flops=2 * rows * width * count * heads[0].shape[1], bytes_accessed=6 << 20, transcendentals=0
        ),
    )(resid, gain, *heads, *weights)


def hidden_kernel(n_rows, n_parts, starts_ref, *refs):
    row_refs, part_refs = refs[:n_rows], refs[n_rows : n_rows + n_parts]
    hidden_ref, rows, weight, row_sems, part_sems = refs[n_rows + n_parts :]
    copies = []
    height = row_refs[0].shape[0]
    for i, ref in enumerate(row_refs):
        copies.append(pltpu.make_async_copy(ref, rows.at[pl.ds(i * height, height)], row_sems.at[i]))
    for i, ref in enumerate(part_refs):
        start = pl.multiple_of(starts_ref[i], ref.shape[0])
        copies.append(pltpu.make_async_copy(ref, weight.at[pl.ds(start, ref.shape[0])], part_sems.at[i]))
    for copy in copies[n_rows:] + copies[:n_rows]:
        copy.start()
    for copy in copies[n_rows:]:
        copy.wait()
    half = hidden_ref.shape[1]
    tile = min(512, rows.shape[0])
    for lower in range(0, rows.shape[0], tile):
        part = pl.ds(lower, tile)
        for i in range(lower // height, (lower + tile) // height):
            copies[i].wait()
        for start in range(0, half, 128):
            size = min(128, half - start)
            both = jnp.dot(
                rows[part, :], weight[:, 2 * start : 2 * (start + size)], preferred_element_type=jnp.float32
            )
            gate, up = both[:, :size], both[:, size:]
            hidden_ref[part, start : start + size] = (gate / (1.0 + jnp.exp(-gate)) * up).astype(jnp.bfloat16)


def hidden_units(starts, row_blocks, parts):
    rows = sum(block.shape[0] for block in row_blocks)
    depth, width = row_blocks[0].shape[1], parts[0].shape[1]
    return pl.pallas_call(
        functools.partial(hidden_kernel, len(row_blocks), len(parts)),
        out_shape=jax.ShapeDtypeStruct((rows, width // 2), jnp.bfloat16),
        in_specs=[SMEM] + [ANY] * (len(row_blocks) + len(parts)),
        out_specs=VMEM,
        scratch_shapes=[
            pltpu.VMEM((rows, depth), jnp.bfloat16),
            pltpu.VMEM((depth, width), jnp.bfloat16),
            pltpu.SemaphoreType.DMA((len(row_blocks),)),
            pltpu.SemaphoreType.DMA((len(parts),)),
        ],
        cost_estimate=pl.CostEstimate(
            flops=2 * rows * width * depth, bytes_accessed=11 << 20, transcendentals=rows * width // 2
        ),
        compiler_params=pltpu.CompilerParams(vmem_limit_bytes=40 << 20),
    )(starts, *row_blocks, *parts)


def down_kernel(n_parts, starts_ref, hidden_ref, *refs):
    part_refs, (keep_ref, send_ref, weight, sems) = refs[:n_parts], refs[n_parts:]
    copies = []
    for i, ref in enumerate(part_refs):
        start = pl.multiple_of(starts_ref[i], ref.shape[1]) if n_parts > 1 else 0
        copies.append(pltpu.make_async_copy(ref, weight.at[:, pl.ds(start, ref.shape[1])], sems.at[i]))
    for copy in copies:
        copy.start()
    for copy in copies:
        copy.wait()
    keep = keep_ref.shape[0]
    tile = min(256, keep)
    for target, base in ((send_ref, keep), (keep_ref, 0)):
        for lower in range(0, keep, tile):
            target[pl.ds(lower, tile), :] = jnp.dot(
                hidden_ref[pl.ds(base + lower, tile), :], weight[...], preferred_element_type=jnp.float32
            ).astype(jnp.bfloat16)


def down_rows(starts, hidden, parts):
    rows, depth = hidden.shape
    width = sum(part.shape[1] for part in parts)
    shape = jax.ShapeDtypeStruct((rows // 2, width), jnp.bfloat16)
    return pl.pallas_call(
        functools.partial(down_kernel, len(parts)),
        out_shape=(shape, shape),
        in_specs=[SMEM, VMEM] + [ANY] * len(parts),
        out_specs=(VMEM, VMEM),
        scratch_shapes=[
            pltpu.VMEM((depth, width), jnp.bfloat16),
            pltpu.SemaphoreType.DMA((len(parts),)),
        ],
        cost_estimate=pl.CostEstimate(
            flops=2 * rows * width * depth, bytes_accessed=4 << 20, transcendentals=0
        ),
        compiler_params=pltpu.CompilerParams(vmem_limit_bytes=24 << 20),
    )(starts, hidden, *parts)


def finish_kernel(plan, per_chunk, bases_ref, middle_ref, *refs):
    out_ref = refs[-1]
    for chunk, (strips, pitch, shift) in enumerate(plan):
        totals = refs[chunk * per_chunk : (chunk + 1) * per_chunk]
        width = totals[0].shape[1] // strips
        for strip in range(strips):
            start = bases_ref[chunk] + (strip * pitch + shift)
            cols = pl.ds(pl.multiple_of(start, width), width)
            total = middle_ref[:, cols]
            for ref in totals:
                total += ref[:, strip * width : (strip + 1) * width].astype(jnp.float32)
            out_ref[:, cols] = total.astype(jnp.bfloat16)


def finish(plan, bases, middle, chunks):
    return pl.pallas_call(
        functools.partial(finish_kernel, plan, len(chunks[0])),
        out_shape=jax.ShapeDtypeStruct(middle.shape, jnp.bfloat16),
        in_specs=[SMEM] + [VMEM] * (1 + len(chunks) * len(chunks[0])),
        out_specs=VMEM,
        cost_estimate=pl.CostEstimate(
            flops=8 * middle.size, bytes_accessed=8 * middle.size, transcendentals=0
        ),
    )(bases, middle, *[block for chunk in chunks for block in chunk])


def lay_out(parts, starts, axis):
    total = sum(part.shape[axis] for part in parts)
    shape = list(parts[0].shape)
    shape[axis] = total
    whole = jnp.zeros(shape, parts[0].dtype)
    for part, start in zip(parts, starts):
        whole = lax.dynamic_update_slice_in_dim(whole, part, start, axis)
    return whole


def y_count(n_sp):
    return 1 << ((n_sp.bit_length() - 1) // 2)


def shards(q_proj, k_proj, v_proj, doc_ids, sinks, resid, w_out, norm_gain, w_gate, w_up, w_down):
    n_sp, n_tp = lax.axis_size("sp"), lax.axis_size("tp")
    n_y = y_count(n_sp)
    n_z = n_sp // n_y
    sp = lax.axis_index("sp")
    z = sp // n_y
    depth, piece = w_gate.shape[0], w_down.shape[1]

    info = (z % 2).astype(jnp.int32)[None]
    gu_cuts = 2 if depth % 32 == 0 else 1
    down_cuts = 2 if piece % 256 == 0 else 1
    gu_half = pack_gate_up(info, w_gate, w_up, gu_cuts)
    down_half = split_down(info, w_down, down_cuts)

    gu_parts, gu_starts = [], []
    for dz in range(n_z):
        cuts = 1 if dz < 2 else gu_cuts
        height = depth // cuts
        for cut in range(cuts):
            held = swap(gu_half[dz % 2][cut + 1 if dz >= 2 else 0], dz * n_y)
            for dy in range(n_y):
                gu_parts.append(swap(held, dy))
                gu_starts.append((sp ^ (dz * n_y + dy)) * depth + cut * height)
    down, cuts_of = {}, {}
    for dz in range(n_z):
        cuts = cuts_of[dz // 2] = 1 if dz < 2 else down_cuts
        for cut in range(cuts):
            held = swap(down_half[dz % 2][cut + 1 if dz >= 2 else 0], dz * n_y)
            for dy in range(n_y):
                down[dz, cut, dy] = swap(held, dy)

    attended = attention(q_proj, k_proj, v_proj, doc_ids, sinks)

    out_blocks = {}
    for t in range(0, n_tp, 2):
        out_blocks[t] = swap(w_out, 0, t)
        out_blocks[t + 1] = swap(out_blocks[t], 0, 1)
    heads = [swap(attended[t], 0, t) for t in range(n_tp)]
    middle, normed = project(
        resid, norm_gain[None, :], heads, [out_blocks[t] for t in range(n_tp)]
    )

    rows = {(0, 0): normed, (1, 0): swap(normed, n_y)}
    for t in range(2, n_tp, 2):
        for a in (0, 1):
            rows[a, t] = swap(rows[a, 0], 0, t)
    for (a, t), block in list(rows.items()):
        rows[a, t + 1] = swap(block, 0, 1)
    order = [(a, t + c) for c in (0, 1) for a in (0, 1) for t in range(0, n_tp, 2)]

    hidden = hidden_units(
        jnp.stack(gu_starts).astype(jnp.int32), [rows[key] for key in order], gu_parts
    )

    plan, bases, chunks = [], [], []
    span = 2 * n_y * piece
    for pair, cuts in cuts_of.items():
        width = piece // cuts
        for cut in range(cuts):
            keys = [(2 * pair + b, dy) for b in (0, 1) for dy in range(n_y)]
            starts = [((sp ^ (dz * n_y + dy)) % (2 * n_y)) * width for dz, dy in keys]
            parts = [down[dz, cut, dy] for dz, dy in keys]
            if width % 128:
                parts, starts = [lay_out(parts, starts, 1)], [sp * 0]
            keep, send = down_rows(jnp.stack(starts).astype(jnp.int32), hidden, parts)
            other = swap(send, 0, 1)
            totals = merge(keep, other, len(order) // 2)
            plan.append((1, span, 0) if cuts == 1 else (2 * n_y, piece, cut * width))
            bases.append((z // 2 ^ pair) * span)
            chunks.append([swap(totals[i], a * n_y, t) for i, (a, t) in enumerate(order[: len(order) // 2])])
    return finish(tuple(plan), jnp.stack(bases).astype(jnp.int32), middle, chunks)


def solution(mesh):
    placed = (
        P("sp", "tp"),
        P("sp", "tp"),
        P("sp", "tp"),
        P("sp"),
        P("tp"),
        P(("sp", "tp"), None),
        P("tp", None),
        P(),
        P("sp", "tp"),
        P("sp", "tp"),
        P("tp", "sp"),
    )

    return jax.shard_map(shards, mesh=mesh, in_specs=placed, out_specs=P(("sp", "tp"), None), check_vma=False)
```

```python
import functools

import jax
import jax.numpy as jnp
from jax import lax
from jax.experimental import pallas as pl
from jax.experimental.pallas import tpu as pltpu
from jax.sharding import PartitionSpec as P


HEAD = 64
WINDOW = 128

norm_eps = 1e-06
masked = -1e30


def swap(block, sp_mask=0, tp_mask=0):
    n_sp, n_tp = lax.axis_size("sp"), lax.axis_size("tp")
    if sp_mask and tp_mask:
        axis = ("sp", "tp")
        pairs = [
            (s * n_tp + t, (s ^ sp_mask) * n_tp + (t ^ tp_mask))
            for s in range(n_sp)
            for t in range(n_tp)
        ]
    elif sp_mask:
        axis, pairs = "sp", [(s, s ^ sp_mask) for s in range(n_sp)]
    elif tp_mask:
        axis, pairs = "tp", [(t, t ^ tp_mask) for t in range(n_tp)]
    else:
        return block
    return lax.ppermute(block, axis, pairs)


def edge_kernel(place_ref, docs_ref, k_ref, v_ref, kv_first_ref, kv_second_ref, doc_first_ref, doc_second_ref):
    even = place_ref[0] & 1 == 0
    last = k_ref.shape[0] - WINDOW
    kv_cols = k_ref.shape[1]
    for ref, cols in ((k_ref, slice(0, kv_cols)), (v_ref, slice(kv_cols, 2 * kv_cols))):
        head, tail = ref[:WINDOW, :], ref[last:, :]
        kv_first_ref[:, cols] = jnp.where(even, tail, head)
        kv_second_ref[:, cols] = jnp.where(even, head, tail)
    head, tail = docs_ref[:, :WINDOW], docs_ref[:, last:]
    doc_first_ref[...] = jnp.where(even, tail, head)
    doc_second_ref[...] = jnp.where(even, head, tail)


def attention_kernel(n_sp, n_out, place_ref, sinks_ref, docs_ref, q_ref, k_ref, v_ref, *refs):
    first_ref, second_ref, doc_first_ref, doc_second_ref = refs[:4]
    out_refs, attended = refs[4 : 4 + n_out], refs[4 + n_out]
    sp = place_ref[0]
    kv_cols = k_ref.shape[1]
    kv_heads = kv_cols // HEAD
    groups = q_ref.shape[1] // kv_cols
    count = q_ref.shape[0] // WINDOW
    span = 3 * WINDOW
    shape = (WINDOW, span)
    even = sp & 1 == 0
    offset = lax.broadcasted_iota(jnp.int32, shape, 1) - lax.broadcasted_iota(jnp.int32, shape, 0)
    near = (offset >= 0) & (offset <= 2 * WINDOW)
    ones = jnp.ones((span, HEAD), jnp.bfloat16)
    doc_first, doc_second = doc_first_ref[...], doc_second_ref[...]
    docs = jnp.concatenate(
        [
            jnp.where(sp == 0, -1, jnp.where(even, doc_second, doc_first)),
            docs_ref[...],
            jnp.where(sp == n_sp - 1, -1, jnp.where(even, doc_first, doc_second)),
        ],
        axis=1,
    )

    def band(own_ref, column, block):
        cols = slice(column, column + kv_cols)
        pieces = []
        for i in range(block - 1, block + 2):
            if 0 <= i < count:
                pieces.append(own_ref[i * WINDOW : (i + 1) * WINDOW, :])
            elif i < 0:
                pieces.append(jnp.where(even, second_ref[:, cols], first_ref[:, cols]))
            else:
                pieces.append(jnp.where(even, first_ref[:, cols], second_ref[:, cols]))
        return jnp.concatenate(pieces, axis=0)

    for block in range(count):
        rows = slice(block * WINDOW, (block + 1) * WINDOW)
        own_docs = docs[:, (block + 1) * WINDOW : (block + 2) * WINDOW]
        query_docs = jnp.broadcast_to(own_docs, (WINDOW, WINDOW)).T
        band_docs = docs[:, block * WINDOW : block * WINDOW + span]
        valid = near & (jnp.concatenate([query_docs] * 3, axis=1) == band_docs)
        keys, values = band(k_ref, 0, block), band(v_ref, kv_cols, block)
        queries = q_ref[rows, :] * HEAD ** (-0.5)
        outs = []
        for head in range(kv_heads):
            cols = slice(head * HEAD, (head + 1) * HEAD)
            key = keys[:, cols]
            value = jnp.concatenate([values[:, cols], ones], axis=1)
            for group in range(groups):
                index = head * groups + group
                scores = lax.dot_general(
                    queries[:, index * HEAD : (index + 1) * HEAD],
                    key,
                    (((1,), (1,)), ((), ())),
                    preferred_element_type=jnp.float32,
                )
                scores = jnp.where(valid, scores, masked)
                sink = sinks_ref[index]
                top = jnp.maximum(jnp.max(scores, axis=-1, keepdims=True), sink)
                expd = jnp.exp(scores - top).astype(jnp.bfloat16)
                both = jnp.dot(expd, value, preferred_element_type=jnp.float32)
                outs.append(both[:, :HEAD] / (both[:, HEAD:] + jnp.exp(sink - top)))
        attended[rows, :] = jnp.concatenate(outs, axis=1).astype(jnp.bfloat16)
    height = out_refs[0].shape[0]
    for i, out_ref in enumerate(out_refs):
        out_ref[...] = attended[pl.ds(pl.multiple_of((place_ref[1] ^ i) * height, height), height), :]


def attention(place, q_proj, k_proj, v_proj, doc_ids, sinks):
    tok_rows, kv_cols = k_proj.shape
    n_tp, n_sp = lax.axis_size("tp"), lax.axis_size("sp")
    doc_ids = doc_ids[None, :]
    kv_edge = jax.ShapeDtypeStruct((WINDOW, 2 * kv_cols), jnp.bfloat16)
    doc_edge = jax.ShapeDtypeStruct((1, WINDOW), jnp.int32)
    kv_first, kv_second, doc_first, doc_second = pl.pallas_call(
        edge_kernel,
        out_shape=(kv_edge, kv_edge, doc_edge, doc_edge),
        in_specs=[SMEM] + [VMEM] * 3,
        out_specs=(VMEM,) * 4,
        compiler_params=room(4),
    )(place, doc_ids, k_proj, v_proj)

    def trade(name, block):
        low = int(name.endswith("second"))
        pairs = [(i, i + 1) for i in range(low, n_sp - 1, 2)]
        return lax.ppermute(block, "sp", pairs + [(b, a) for a, b in pairs])

    edges = [trade("kv_first", kv_first), trade("kv_second", kv_second)]
    edges += [trade("doc_first", doc_first), trade("doc_second", doc_second)]
    own = jax.ShapeDtypeStruct((tok_rows // n_tp, q_proj.shape[1]), jnp.bfloat16)
    return pl.pallas_call(
        functools.partial(attention_kernel, n_sp, n_tp),
        out_shape=(own,) * n_tp,
        in_specs=[SMEM] * 2 + [VMEM] * 8,
        out_specs=(VMEM,) * n_tp,
        scratch_shapes=[pltpu.VMEM(q_proj.shape, jnp.bfloat16)],
        compiler_params=room(8),
        cost_estimate=pl.CostEstimate(
            flops=12 * tok_rows * WINDOW * q_proj.shape[1],
            bytes_accessed=1 << 20,
            transcendentals=0,
        ),
    )(place, sinks, doc_ids, q_proj, k_proj, v_proj, *edges)


SMEM = pl.BlockSpec(memory_space=pltpu.SMEM)
VMEM = pl.BlockSpec(memory_space=pltpu.VMEM)
ANY = pl.BlockSpec(memory_space=pl.ANY)
HBM = pl.BlockSpec(memory_space=pltpu.HBM)


def room(mebibytes):
    return pltpu.CompilerParams(vmem_limit_bytes=mebibytes << 20)


def pack_kernel(half, y_bits, wanted, place_ref, gate_ref, up_ref, *refs):
    whole = half // 128 * 128

    def fill(source, chosen):
        lower = source * half

        def store(start, value):
            for (_, low, high), ref in chosen:
                ref[:, start : start + value.shape[1]] = value[low:high]

        for start in range(0, whole, 128):
            for ref, shift in ((gate_ref, 0), (up_ref, 128)):
                store(2 * start + shift, ref[:, lower + start : lower + start + 128])
        if half > whole:
            rest = [ref[:, lower + whole : lower + half] for ref in (gate_ref, up_ref)]
            store(2 * whole, jnp.concatenate(rest, axis=1))

    for source in (0, 1):
        for parity in (0, 1):
            chosen = [(want, ref) for want, ref in zip(wanted, refs) if want[0] == parity]

            @pl.when((place_ref[0] >> y_bits) & 1 == source ^ parity)
            def _():
                fill(source, chosen)


def pack_gate_up(place, y_bits, w_gate, w_up, wanted):
    depth, width = w_gate.shape
    return pl.pallas_call(
        functools.partial(pack_kernel, width // 2, y_bits, wanted),
        out_shape=tuple(
            jax.ShapeDtypeStruct((high - low, width), jnp.bfloat16) for _, low, high in wanted
        ),
        in_specs=[SMEM, VMEM, VMEM],
        out_specs=(VMEM,) * len(wanted),
        compiler_params=room(8),
        cost_estimate=pl.CostEstimate(flops=4 * depth * width, bytes_accessed=6 * w_gate.size, transcendentals=0),
    )(place, w_gate, w_up)


def split_kernel(far_cuts, y_bits, place_ref, down_ref, *refs):
    half = refs[0].shape[0]
    for parity in (0, 1):
        targets = refs[parity * (1 + far_cuts) : (parity + 1) * (1 + far_cuts)]
        rows = pl.ds(pl.multiple_of(((place_ref[0] >> y_bits) & 1 ^ parity) * half, half), half)
        value = down_ref[rows, :]
        width = value.shape[1] // far_cuts
        targets[0][...] = value
        for cut in range(far_cuts):
            targets[1 + cut][...] = value[:, cut * width : (cut + 1) * width]


def split_down(place, y_bits, w_down, far_cuts):
    depth, width = w_down.shape
    near = jax.ShapeDtypeStruct((depth // 2, width), jnp.bfloat16)
    far = jax.ShapeDtypeStruct((depth // 2, width // far_cuts), jnp.bfloat16)
    halves = pl.pallas_call(
        functools.partial(split_kernel, far_cuts, y_bits),
        out_shape=((near,) + (far,) * far_cuts) * 2,
        in_specs=[SMEM, VMEM],
        out_specs=(VMEM,) * (2 * (1 + far_cuts)),
        compiler_params=room(8),
        cost_estimate=pl.CostEstimate(flops=depth * width, bytes_accessed=8 * depth * width, transcendentals=0),
    )(place, w_down)
    return halves[: 1 + far_cuts], halves[1 + far_cuts :]


def merge_kernel(keep_ref, other_ref, *out_refs):
    height = out_refs[0].shape[0]
    for i, out_ref in enumerate(out_refs):
        rows = pl.ds(i * height, height)
        total = keep_ref[rows, :].astype(jnp.float32) + other_ref[rows, :].astype(jnp.float32)
        out_ref[...] = total.astype(jnp.bfloat16)


def merge(keep, other, count):
    part = jax.ShapeDtypeStruct((keep.shape[0] // count, keep.shape[1]), jnp.bfloat16)
    return pl.pallas_call(
        merge_kernel,
        out_shape=(part,) * count,
        in_specs=[VMEM] * 2,
        out_specs=(VMEM,) * count,
        compiler_params=room(8),
        cost_estimate=pl.CostEstimate(flops=keep.size, bytes_accessed=6 * keep.size, transcendentals=0),
    )(keep, other)


def project_kernel(count, resid_ref, gain_ref, *refs):
    heads, weights, (middle_ref, normed_ref) = refs[:count], refs[count : 2 * count], refs[2 * count :]
    width = middle_ref.shape[1]
    tile = min(512, width)
    squares = jnp.zeros((middle_ref.shape[0], 1), jnp.float32)
    for lower in range(0, width, tile):
        cols = pl.ds(lower, tile)
        total = resid_ref[:, cols].astype(jnp.float32)
        for head, weight in zip(heads, weights):
            total += jnp.dot(head[...], weight[:, cols], preferred_element_type=jnp.float32)
        middle_ref[:, cols] = total
        squares += jnp.sum(total * total, axis=-1, keepdims=True)
    factor = lax.rsqrt(squares / width + norm_eps)
    for lower in range(0, width, tile):
        cols = pl.ds(lower, tile)
        normed_ref[:, cols] = (middle_ref[:, cols] * factor * gain_ref[:, cols]).astype(jnp.bfloat16)


def project(resid, gain, heads, weights):
    rows, width = resid.shape
    count = len(heads)
    return pl.pallas_call(
        functools.partial(project_kernel, count),
        out_shape=(
            jax.ShapeDtypeStruct((rows, width), jnp.float32),
            jax.ShapeDtypeStruct((rows, width), jnp.bfloat16),
        ),
        in_specs=[VMEM] * (2 + 2 * count),
        out_specs=(VMEM, VMEM),
        compiler_params=room(12),
        cost_estimate=pl.CostEstimate(
            flops=2 * rows * width * count * heads[0].shape[1], bytes_accessed=6 << 20, transcendentals=0
        ),
    )(resid, gain, *heads, *weights)


def hidden_kernel(n_rows, pair_bits, groups, with_total, last, place_ref, *refs):
    counts = [len(starts) for _, starts in groups]
    row_refs, refs = refs[:n_rows], refs[n_rows:]
    part_refs, refs = refs[: sum(counts)], refs[sum(counts) :]
    if with_total:
        total_ref, refs = refs[0], refs[1:]
    out_ref, rows, weight, row_sems, part_sems = refs
    pairs, span = len(counts), weight.shape[1]
    height = row_refs[0].shape[0]
    row_copies, part_copies = [], []
    index = 0
    for pair, count in enumerate(counts):
        columns = pl.ds(pl.multiple_of(((place_ref[0] >> pair_bits) ^ groups[pair][0]) * span, span), span)
        for i, ref in enumerate(row_refs):
            row_copies.append(
                pltpu.make_async_copy(
                    ref.at[:, columns], rows.at[pair, pl.ds(i * height, height)], row_sems.at[pair, i]
                )
            )
        for (mask, scale, shift), ref in zip(groups[pair][1], part_refs[index : index + count]):
            within = (place_ref[0] ^ mask) & ((1 << pair_bits) - 1)
            start = pl.multiple_of(within * scale + shift, ref.shape[0])
            part_copies.append(
                pltpu.make_async_copy(ref, weight.at[pair, pl.ds(start, ref.shape[0])], part_sems.at[index])
            )
            index += 1
    for copy in part_copies + row_copies:
        copy.start()
    for copy in part_copies:
        copy.wait()
    total_rows, width = rows.shape[1], weight.shape[2]
    tile = min(512, total_rows)
    for lower in range(0, total_rows, tile):
        part = pl.ds(lower, tile)
        for i in range(lower // height, (lower + tile) // height):
            for pair in range(pairs):
                row_copies[pair * n_rows + i].wait()
        for start in range(0, width, 256):
            size = min(256, width - start)
            cols = slice(start, start + size)
            both = total_ref[part, cols] if with_total else 0.0
            for pair in range(pairs):
                both += jnp.dot(rows[pair, part, :], weight[pair, :, cols], preferred_element_type=jnp.float32)
            if last:
                gate, up = both[:, : size // 2], both[:, size // 2 :]
                out_ref[part, start // 2 : (start + size) // 2] = (gate / (1.0 + jnp.exp(-gate)) * up).astype(
                    jnp.bfloat16
                )
            else:
                out_ref[part, cols] = both


def hidden_units(place, pair_bits, groups, row_blocks, parts, total, last):
    rows = sum(block.shape[0] for block in row_blocks)
    width = parts[0][0].shape[1]
    span = sum(part.shape[0] for part in parts[0])
    flat = [part for group in parts for part in group]
    out = jax.ShapeDtypeStruct((rows, width // 2), jnp.bfloat16)
    if not last:
        out = jax.ShapeDtypeStruct((rows, width), jnp.float32)
    return pl.pallas_call(
        functools.partial(
            hidden_kernel, len(row_blocks), pair_bits, groups, total is not None, last
        ),
        out_shape=out,
        in_specs=[SMEM]
        + [HBM] * (len(row_blocks) + len(flat))
        + ([VMEM] if total is not None else []),
        out_specs=VMEM,
        scratch_shapes=[
            pltpu.VMEM((len(parts), rows, span), jnp.bfloat16),
            pltpu.VMEM((len(parts), span, width), jnp.bfloat16),
            pltpu.SemaphoreType.DMA((len(parts), len(row_blocks))),
            pltpu.SemaphoreType.DMA((len(flat),)),
        ],
        cost_estimate=pl.CostEstimate(
            flops=2 * rows * width * span * len(parts),
            bytes_accessed=8 << 20,
            transcendentals=0,
        ),
        compiler_params=room(12),
    )(place, *row_blocks, *flat, *([total] if total is not None else []))


def down_kernel(pair_bits, masks, place_ref, hidden_ref, *refs):
    n_parts = len(masks)
    part_refs, (keep_ref, send_ref, weight, sems) = refs[:n_parts], refs[n_parts:]
    copies = []
    for i, ref in enumerate(part_refs):
        start = 0
        if n_parts > 1:
            within = (place_ref[0] ^ masks[i]) & ((1 << pair_bits) - 1)
            start = pl.multiple_of(within * ref.shape[1], ref.shape[1])
        copies.append(pltpu.make_async_copy(ref, weight.at[:, pl.ds(start, ref.shape[1])], sems.at[i]))
    for copy in copies:
        copy.start()
    for copy in copies:
        copy.wait()
    keep = keep_ref.shape[0]
    tile = min(256, keep)
    for target, base in ((send_ref, keep), (keep_ref, 0)):
        for lower in range(0, keep, tile):
            target[pl.ds(lower, tile), :] = jnp.dot(
                hidden_ref[pl.ds(base + lower, tile), :], weight[...], preferred_element_type=jnp.float32
            ).astype(jnp.bfloat16)


def down_rows(place, pair_bits, masks, hidden, parts):
    rows, depth = hidden.shape
    width = sum(part.shape[1] for part in parts)
    shape = jax.ShapeDtypeStruct((rows // 2, width), jnp.bfloat16)
    return pl.pallas_call(
        functools.partial(down_kernel, pair_bits, masks),
        out_shape=(shape, shape),
        in_specs=[SMEM, VMEM] + [HBM] * len(parts),
        out_specs=(VMEM, VMEM),
        scratch_shapes=[
            pltpu.VMEM((depth, width), jnp.bfloat16),
            pltpu.SemaphoreType.DMA((len(parts),)),
        ],
        cost_estimate=pl.CostEstimate(
            flops=2 * rows * width * depth, bytes_accessed=4 << 20, transcendentals=0
        ),
        compiler_params=room(8),
    )(place, hidden, *parts)


def finish_kernel(pair_bits, plan, per_chunk, place_ref, middle_ref, *refs):
    out_ref = refs[-1]
    for chunk, (pair, span, strips, pitch, shift) in enumerate(plan):
        base = ((place_ref[0] >> pair_bits) ^ pair) * span
        totals = refs[chunk * per_chunk : (chunk + 1) * per_chunk]
        width = totals[0].shape[1] // strips
        for strip in range(strips):
            start = base + (strip * pitch + shift)
            cols = pl.ds(pl.multiple_of(start, width), width)
            total = middle_ref[:, cols]
            for ref in totals:
                total += ref[:, strip * width : (strip + 1) * width].astype(jnp.float32)
            out_ref[:, cols] = total.astype(jnp.bfloat16)


def finish(place, pair_bits, plan, middle, chunks):
    count = len(chunks) * len(chunks[0])
    return pl.pallas_call(
        functools.partial(finish_kernel, pair_bits, plan, len(chunks[0])),
        out_shape=jax.ShapeDtypeStruct(middle.shape, jnp.bfloat16),
        in_specs=[SMEM] + [VMEM] * (1 + count),
        out_specs=VMEM,
        compiler_params=room(8),
        cost_estimate=pl.CostEstimate(
            flops=8 * middle.size, bytes_accessed=8 * middle.size, transcendentals=0
        ),
    )(place, middle, *[block for chunk in chunks for block in chunk])


def lay_out(parts, starts, axis):
    total = sum(part.shape[axis] for part in parts)
    shape = list(parts[0].shape)
    shape[axis] = total
    whole = jnp.zeros(shape, parts[0].dtype)
    for part, start in zip(parts, starts):
        whole = lax.dynamic_update_slice_in_dim(whole, part, start, axis)
    return whole


def y_count(n_sp):
    return 1 << ((n_sp.bit_length() - 1) // 2)


def shards(q_proj, k_proj, v_proj, doc_ids, sinks, resid, w_out, norm_gain, w_gate, w_up, w_down):
    n_sp, n_tp = lax.axis_size("sp"), lax.axis_size("tp")
    n_y = y_count(n_sp)
    n_z = n_sp // n_y
    y_bits = n_y.bit_length() - 1
    place = jnp.stack([lax.axis_index("sp"), lax.axis_index("tp")]).astype(jnp.int32)
    depth, piece = w_gate.shape[0], w_down.shape[1]

    gu_cuts = 2 if depth % 32 == 0 else 1
    down_cuts = 2 if piece % 256 == 0 else 1
    step = depth // gu_cuts
    cuts = [(cut * step, (cut + 1) * step) for cut in range(gu_cuts)]
    wanted = [[(1, 0, depth), (0, *cuts[0]), (1, *cuts[0])], [(0, 0, depth)]]
    wanted[1] += [(parity, *cut) for cut in cuts[1:] for parity in (0, 1)]
    gu_half = {}
    for group in wanted:
        packed = pack_gate_up(place, y_bits, w_gate, w_up, tuple(group))
        for (parity, low, high), value in zip(group, packed):
            gu_half[parity, low, high] = value
    down_half = split_down(place, y_bits, w_down, down_cuts)

    gu = {}
    for dz in range(n_z):
        cuts = 1 if dz < 2 else gu_cuts
        height = depth // cuts
        for cut in range(cuts):
            held = swap(gu_half[dz % 2, cut * height, (cut + 1) * height], dz * n_y)
            for dy in range(n_y):
                start = (dz * n_y + dy, depth, cut * height)
                gu.setdefault(dz // 2, []).append((swap(held, dy), start))
    down, cuts_of = {}, {}
    for dz in range(n_z):
        cuts = cuts_of[dz // 2] = 1 if dz < 2 else down_cuts
        for cut in range(cuts):
            held = swap(down_half[dz % 2][cut + 1 if dz >= 2 else 0], dz * n_y)
            for dy in range(n_y):
                down[dz, cut, dy] = swap(held, dy)

    attended = attention(place, q_proj, k_proj, v_proj, doc_ids, sinks)

    out_blocks = {}
    for t in range(0, n_tp, 2):
        out_blocks[t] = swap(w_out, 0, t)
        out_blocks[t + 1] = swap(out_blocks[t], 0, 1)
    heads = [swap(attended[t], 0, t) for t in range(n_tp)]
    middle, normed = project(
        resid, norm_gain[None, :], heads, [out_blocks[t] for t in range(n_tp)]
    )

    rows = {(0, 0): normed, (1, 0): swap(normed, n_y)}
    for t in range(2, n_tp, 2):
        for a in (0, 1):
            rows[a, t] = swap(rows[a, 0], 0, t)
    for (a, t), block in list(rows.items()):
        rows[a, t + 1] = swap(block, 0, 1)
    order = [(a, t + c) for c in (0, 1) for a in (0, 1) for t in range(0, n_tp, 2)]

    blocks = [rows[key] for key in order]
    hidden = None
    for pairs in ([0], list(range(1, n_z // 2))):
        hidden = hidden_units(
            place,
            y_bits + 1,
            [(pair, [start for _, start in gu[pair]]) for pair in pairs],
            blocks,
            [[part for part, _ in gu[pair]] for pair in pairs],
            hidden,
            pairs[0] > 0,
        )

    span = 2 * n_y * piece
    plan, chunks = [], []
    for pair, cuts in cuts_of.items():
        width = piece // cuts
        for cut in range(cuts):
            keys = [(2 * pair + b, dy) for b in (0, 1) for dy in range(n_y)]
            masks = [dz * n_y + dy for dz, dy in keys]
            parts = [down[dz, cut, dy] for dz, dy in keys]
            if width % 128:
                starts = [((place[0] ^ mask) % (2 * n_y)) * width for mask in masks]
                parts, masks = [lay_out(parts, starts, 1)], [0]
            keep, send = down_rows(place, y_bits + 1, masks, hidden, parts)
            other = swap(send, 0, 1)
            totals = merge(keep, other, len(order) // 2)
            plan.append((pair, span) + ((1, span, 0) if cuts == 1 else (2 * n_y, piece, cut * width)))
            chunks.append([swap(totals[i], a * n_y, t) for i, (a, t) in enumerate(order[: len(order) // 2])])
    return finish(place, y_bits + 1, plan, middle, chunks)


def solution(mesh):
    placed = (
        P("sp", "tp"),
        P("sp", "tp"),
        P("sp", "tp"),
        P("sp"),
        P("tp"),
        P(("sp", "tp"), None),
        P("tp", None),
        P(),
        P("sp", "tp"),
        P("sp", "tp"),
        P("tp", "sp"),
    )

    return jax.shard_map(shards, mesh=mesh, in_specs=placed, out_specs=P(("sp", "tp"), None), check_vma=False)
```

```python
import functools

import jax
import jax.numpy as jnp
from jax import lax
from jax.experimental import pallas as pl
from jax.experimental.pallas import tpu as pltpu
from jax.sharding import PartitionSpec as P


HEAD = 64
WINDOW = 128

norm_eps = 1e-06
masked = -1e30


def swap(block, sp_mask=0, tp_mask=0):
    n_sp, n_tp = lax.axis_size("sp"), lax.axis_size("tp")
    if sp_mask and tp_mask:
        axis = ("sp", "tp")
        pairs = [
            (s * n_tp + t, (s ^ sp_mask) * n_tp + (t ^ tp_mask))
            for s in range(n_sp)
            for t in range(n_tp)
        ]
    elif sp_mask:
        axis, pairs = "sp", [(s, s ^ sp_mask) for s in range(n_sp)]
    elif tp_mask:
        axis, pairs = "tp", [(t, t ^ tp_mask) for t in range(n_tp)]
    else:
        return block
    return lax.ppermute(block, axis, pairs)


def edge_kernel(place_ref, docs_ref, k_ref, v_ref, *refs):
    kv_first_ref, kv_second_ref, doc_first_ref, doc_second_ref = refs[:4]
    for source, target in zip((docs_ref, k_ref, v_ref), refs[4:]):
        target[...] = source[...]
    even = place_ref[0] & 1 == 0
    last = k_ref.shape[0] - WINDOW
    kv_cols = k_ref.shape[1]
    for ref, cols in ((k_ref, slice(0, kv_cols)), (v_ref, slice(kv_cols, 2 * kv_cols))):
        head, tail = ref[:WINDOW, :], ref[last:, :]
        kv_first_ref[:, cols] = jnp.where(even, tail, head)
        kv_second_ref[:, cols] = jnp.where(even, head, tail)
    head, tail = docs_ref[:, :WINDOW], docs_ref[:, last:]
    doc_first_ref[...] = jnp.where(even, tail, head)
    doc_second_ref[...] = jnp.where(even, head, tail)


def attention_kernel(n_sp, n_out, place_ref, sinks_ref, docs_ref, q_ref, k_ref, v_ref, *refs):
    first_ref, second_ref, doc_first_ref, doc_second_ref = refs[:4]
    out_refs, attended = refs[4 : 4 + n_out], refs[4 + n_out]
    sp = place_ref[0]
    kv_cols = k_ref.shape[1]
    kv_heads = kv_cols // HEAD
    groups = q_ref.shape[1] // kv_cols
    count = q_ref.shape[0] // WINDOW
    span = 3 * WINDOW
    shape = (WINDOW, span)
    even = sp & 1 == 0
    offset = lax.broadcasted_iota(jnp.int32, shape, 1) - lax.broadcasted_iota(jnp.int32, shape, 0)
    near = (offset >= 0) & (offset <= 2 * WINDOW)
    ones = jnp.ones((span, HEAD), jnp.bfloat16)
    doc_first, doc_second = doc_first_ref[...], doc_second_ref[...]
    docs = jnp.concatenate(
        [
            jnp.where(sp == 0, -1, jnp.where(even, doc_second, doc_first)),
            docs_ref[...],
            jnp.where(sp == n_sp - 1, -1, jnp.where(even, doc_first, doc_second)),
        ],
        axis=1,
    )

    def band(own_ref, column, block):
        cols = slice(column, column + kv_cols)
        pieces = []
        for i in range(block - 1, block + 2):
            if 0 <= i < count:
                pieces.append(own_ref[i * WINDOW : (i + 1) * WINDOW, :])
            elif i < 0:
                pieces.append(jnp.where(even, second_ref[:, cols], first_ref[:, cols]))
            else:
                pieces.append(jnp.where(even, first_ref[:, cols], second_ref[:, cols]))
        return jnp.concatenate(pieces, axis=0)

    for block in range(count):
        rows = slice(block * WINDOW, (block + 1) * WINDOW)
        own_docs = docs[:, (block + 1) * WINDOW : (block + 2) * WINDOW]
        query_docs = jnp.broadcast_to(own_docs, (WINDOW, WINDOW)).T
        band_docs = docs[:, block * WINDOW : block * WINDOW + span]
        valid = near & (jnp.concatenate([query_docs] * 3, axis=1) == band_docs)
        keys, values = band(k_ref, 0, block), band(v_ref, kv_cols, block)
        queries = q_ref[rows, :] * HEAD ** (-0.5)
        outs = []
        for head in range(kv_heads):
            cols = slice(head * HEAD, (head + 1) * HEAD)
            key = keys[:, cols]
            value = jnp.concatenate([values[:, cols], ones], axis=1)
            for group in range(groups):
                index = head * groups + group
                scores = lax.dot_general(
                    queries[:, index * HEAD : (index + 1) * HEAD],
                    key,
                    (((1,), (1,)), ((), ())),
                    preferred_element_type=jnp.float32,
                )
                scores = jnp.where(valid, scores, masked)
                sink = sinks_ref[index]
                top = jnp.maximum(jnp.max(scores, axis=-1, keepdims=True), sink)
                expd = jnp.exp(scores - top).astype(jnp.bfloat16)
                both = jnp.dot(expd, value, preferred_element_type=jnp.float32)
                outs.append(both[:, :HEAD] / (both[:, HEAD:] + jnp.exp(sink - top)))
        attended[rows, :] = jnp.concatenate(outs, axis=1).astype(jnp.bfloat16)
    height = out_refs[0].shape[0]
    for i, out_ref in enumerate(out_refs):
        out_ref[...] = attended[pl.ds(pl.multiple_of((place_ref[1] ^ i) * height, height), height), :]


def attention(place, q_proj, k_proj, v_proj, doc_ids, sinks):
    tok_rows, kv_cols = k_proj.shape
    n_tp, n_sp = lax.axis_size("tp"), lax.axis_size("sp")
    doc_ids = doc_ids[None, :]
    kv_edge = jax.ShapeDtypeStruct((WINDOW, 2 * kv_cols), jnp.bfloat16)
    doc_edge = jax.ShapeDtypeStruct((1, WINDOW), jnp.int32)
    same = [jax.ShapeDtypeStruct(array.shape, array.dtype) for array in (doc_ids, k_proj, v_proj)]
    kv_first, kv_second, doc_first, doc_second, doc_ids, k_proj, v_proj = pl.pallas_call(
        edge_kernel,
        out_shape=(kv_edge, kv_edge, doc_edge, doc_edge, *same),
        in_specs=[SMEM] + [VMEM] * 3,
        out_specs=(VMEM,) * 7,
        compiler_params=room(4),
    )(place, doc_ids, k_proj, v_proj)

    def trade(name, block):
        low = int(name.endswith("second"))
        pairs = [(i, i + 1) for i in range(low, n_sp - 1, 2)]
        return lax.ppermute(block, "sp", pairs + [(b, a) for a, b in pairs])

    edges = [trade("kv_first", kv_first), trade("kv_second", kv_second)]
    edges += [trade("doc_first", doc_first), trade("doc_second", doc_second)]
    own = jax.ShapeDtypeStruct((tok_rows // n_tp, q_proj.shape[1]), jnp.bfloat16)
    return pl.pallas_call(
        functools.partial(attention_kernel, n_sp, n_tp),
        out_shape=(own,) * n_tp,
        in_specs=[SMEM] * 2 + [VMEM] * 8,
        out_specs=(VMEM,) * n_tp,
        scratch_shapes=[pltpu.VMEM(q_proj.shape, jnp.bfloat16)],
        compiler_params=room(8),
        cost_estimate=pl.CostEstimate(
            flops=12 * tok_rows * WINDOW * q_proj.shape[1],
            bytes_accessed=1 << 20,
            transcendentals=0,
        ),
    )(place, sinks, doc_ids, q_proj, k_proj, v_proj, *edges)


SMEM = pl.BlockSpec(memory_space=pltpu.SMEM)
VMEM = pl.BlockSpec(memory_space=pltpu.VMEM)
ANY = pl.BlockSpec(memory_space=pl.ANY)
HBM = pl.BlockSpec(memory_space=pltpu.HBM)


def room(mebibytes):
    return pltpu.CompilerParams(vmem_limit_bytes=mebibytes << 20)


def pack_kernel(half, y_bits, wanted, place_ref, gate_ref, up_ref, *refs):
    whole = half // 128 * 128

    def fill(source, chosen):
        lower = source * half

        def store(start, value):
            for (_, low, high), ref in chosen:
                ref[:, start : start + value.shape[1]] = value[low:high]

        for start in range(0, whole, 128):
            for ref, shift in ((gate_ref, 0), (up_ref, 128)):
                store(2 * start + shift, ref[:, lower + start : lower + start + 128])
        if half > whole:
            rest = [ref[:, lower + whole : lower + half] for ref in (gate_ref, up_ref)]
            store(2 * whole, jnp.concatenate(rest, axis=1))

    for source in (0, 1):
        for parity in (0, 1):
            chosen = [(want, ref) for want, ref in zip(wanted, refs) if want[0] == parity]

            @pl.when((place_ref[0] >> y_bits) & 1 == source ^ parity)
            def _():
                fill(source, chosen)


def pack_gate_up(place, y_bits, w_gate, w_up, wanted):
    depth, width = w_gate.shape
    return pl.pallas_call(
        functools.partial(pack_kernel, width // 2, y_bits, wanted),
        out_shape=tuple(
            jax.ShapeDtypeStruct((high - low, width), jnp.bfloat16) for _, low, high in wanted
        ),
        in_specs=[SMEM, VMEM, VMEM],
        out_specs=(VMEM,) * len(wanted),
        compiler_params=room(8),
        cost_estimate=pl.CostEstimate(flops=4 * depth * width, bytes_accessed=6 * w_gate.size, transcendentals=0),
    )(place, w_gate, w_up)


def split_kernel(far_cuts, y_bits, place_ref, down_ref, *refs):
    half = refs[0].shape[0]
    for parity in (0, 1):
        targets = refs[parity * (1 + far_cuts) : (parity + 1) * (1 + far_cuts)]
        rows = pl.ds(pl.multiple_of(((place_ref[0] >> y_bits) & 1 ^ parity) * half, half), half)
        value = down_ref[rows, :]
        width = value.shape[1] // far_cuts
        targets[0][...] = value
        for cut in range(far_cuts):
            targets[1 + cut][...] = value[:, cut * width : (cut + 1) * width]


def split_down(place, y_bits, w_down, far_cuts):
    depth, width = w_down.shape
    near = jax.ShapeDtypeStruct((depth // 2, width), jnp.bfloat16)
    far = jax.ShapeDtypeStruct((depth // 2, width // far_cuts), jnp.bfloat16)
    halves = pl.pallas_call(
        functools.partial(split_kernel, far_cuts, y_bits),
        out_shape=((near,) + (far,) * far_cuts) * 2,
        in_specs=[SMEM, VMEM],
        out_specs=(VMEM,) * (2 * (1 + far_cuts)),
        compiler_params=room(8),
        cost_estimate=pl.CostEstimate(flops=depth * width, bytes_accessed=8 * depth * width, transcendentals=0),
    )(place, w_down)
    return halves[: 1 + far_cuts], halves[1 + far_cuts :]


def project_kernel(count, resid_ref, gain_ref, *refs):
    heads, weights, (middle_ref, normed_ref) = refs[:count], refs[count : 2 * count], refs[2 * count :]
    width = middle_ref.shape[1]
    tile = min(512, width)
    squares = jnp.zeros((middle_ref.shape[0], 1), jnp.float32)
    for lower in range(0, width, tile):
        cols = pl.ds(lower, tile)
        total = resid_ref[:, cols].astype(jnp.float32)
        for head, weight in zip(heads, weights):
            total += jnp.dot(head[...], weight[:, cols], preferred_element_type=jnp.float32)
        middle_ref[:, cols] = total
        squares += jnp.sum(total * total, axis=-1, keepdims=True)
    factor = lax.rsqrt(squares / width + norm_eps)
    for lower in range(0, width, tile):
        cols = pl.ds(lower, tile)
        normed_ref[:, cols] = (middle_ref[:, cols] * factor * gain_ref[:, cols]).astype(jnp.bfloat16)


def project(resid, gain, heads, weights):
    rows, width = resid.shape
    count = len(heads)
    return pl.pallas_call(
        functools.partial(project_kernel, count),
        out_shape=(
            jax.ShapeDtypeStruct((rows, width), jnp.float32),
            jax.ShapeDtypeStruct((rows, width), jnp.bfloat16),
        ),
        in_specs=[VMEM] * (2 + 2 * count),
        out_specs=(VMEM, VMEM),
        compiler_params=room(12),
        cost_estimate=pl.CostEstimate(
            flops=2 * rows * width * count * heads[0].shape[1], bytes_accessed=6 << 20, transcendentals=0
        ),
    )(resid, gain, *heads, *weights)


def hidden_kernel(n_rows, pair_bits, groups, with_total, last, place_ref, *refs):
    counts = [len(starts) for _, starts in groups]
    row_refs, refs = refs[:n_rows], refs[n_rows:]
    part_refs, refs = refs[: sum(counts)], refs[sum(counts) :]
    if with_total:
        total_ref, refs = refs[0], refs[1:]
    out_ref, rows, weight, row_sems, part_sems = refs
    pairs, span = len(counts), weight.shape[1]
    height = row_refs[0].shape[0]
    row_copies, part_copies = [], []
    index = 0
    for pair, count in enumerate(counts):
        columns = pl.ds(pl.multiple_of(((place_ref[0] >> pair_bits) ^ groups[pair][0]) * span, span), span)
        for i, ref in enumerate(row_refs):
            row_copies.append(
                pltpu.make_async_copy(
                    ref.at[:, columns], rows.at[pair, pl.ds(i * height, height)], row_sems.at[pair, i]
                )
            )
        for (mask, scale, shift), ref in zip(groups[pair][1], part_refs[index : index + count]):
            within = (place_ref[0] ^ mask) & ((1 << pair_bits) - 1)
            start = pl.multiple_of(within * scale + shift, ref.shape[0])
            part_copies.append(
                pltpu.make_async_copy(ref, weight.at[pair, pl.ds(start, ref.shape[0])], part_sems.at[index])
            )
            index += 1
    for copy in part_copies + row_copies:
        copy.start()
    for copy in part_copies:
        copy.wait()
    total_rows, width = rows.shape[1], weight.shape[2]
    tile = min(512, total_rows)
    for lower in range(0, total_rows, tile):
        part = pl.ds(lower, tile)
        for i in range(lower // height, (lower + tile) // height):
            for pair in range(pairs):
                row_copies[pair * n_rows + i].wait()
        for start in range(0, width, 256):
            size = min(256, width - start)
            cols = slice(start, start + size)
            both = total_ref[part, cols] if with_total else 0.0
            for pair in range(pairs):
                both += jnp.dot(rows[pair, part, :], weight[pair, :, cols], preferred_element_type=jnp.float32)
            if last:
                gate, up = both[:, : size // 2], both[:, size // 2 :]
                out_ref[part, start // 2 : (start + size) // 2] = (gate / (1.0 + jnp.exp(-gate)) * up).astype(
                    jnp.bfloat16
                )
            else:
                out_ref[part, cols] = both


def hidden_units(place, pair_bits, groups, row_blocks, parts, total, last):
    rows = sum(block.shape[0] for block in row_blocks)
    width = parts[0][0].shape[1]
    span = sum(part.shape[0] for part in parts[0])
    flat = [part for group in parts for part in group]
    out = jax.ShapeDtypeStruct((rows, width // 2), jnp.bfloat16)
    if not last:
        out = jax.ShapeDtypeStruct((rows, width), jnp.float32)
    return pl.pallas_call(
        functools.partial(
            hidden_kernel, len(row_blocks), pair_bits, groups, total is not None, last
        ),
        out_shape=out,
        in_specs=[SMEM]
        + [HBM] * (len(row_blocks) + len(flat))
        + ([VMEM] if total is not None else []),
        out_specs=VMEM,
        scratch_shapes=[
            pltpu.VMEM((len(parts), rows, span), jnp.bfloat16),
            pltpu.VMEM((len(parts), span, width), jnp.bfloat16),
            pltpu.SemaphoreType.DMA((len(parts), len(row_blocks))),
            pltpu.SemaphoreType.DMA((len(flat),)),
        ],
        cost_estimate=pl.CostEstimate(
            flops=2 * rows * width * span * len(parts),
            bytes_accessed=8 << 20,
            transcendentals=0,
        ),
        compiler_params=room(12),
    )(place, *row_blocks, *flat, *([total] if total is not None else []))


def down_kernel(pair_bits, masks, base, n_out, place_ref, hidden_ref, *refs):
    part_refs, refs = refs[: len(masks)], refs[len(masks) :]
    other_ref, refs = (refs[0], refs[1:]) if n_out > 1 else (None, refs)
    out_refs, (weight, sems) = refs[:n_out], refs[n_out:]
    copies = []
    for i, ref in enumerate(part_refs):
        start = 0
        if len(masks) > 1:
            within = (place_ref[0] ^ masks[i]) & ((1 << pair_bits) - 1)
            start = pl.multiple_of(within * ref.shape[1], ref.shape[1])
        copies.append(pltpu.make_async_copy(ref, weight.at[:, pl.ds(start, ref.shape[1])], sems.at[i]))
    for copy in copies:
        copy.start()
    for copy in copies:
        copy.wait()
    rows = hidden_ref.shape[0] // 2
    height = rows // n_out
    tile = min(256, rows)
    for lower in range(0, rows, tile):
        total = jnp.dot(
            hidden_ref[pl.ds(base * rows + lower, tile), :], weight[...], preferred_element_type=jnp.float32
        )
        if n_out == 1:
            out_refs[0][pl.ds(lower, tile), :] = total.astype(jnp.bfloat16)
            continue
        total = (total + other_ref[pl.ds(lower, tile), :].astype(jnp.float32)).astype(jnp.bfloat16)
        for start in range(lower, lower + tile, height):
            out_refs[start // height][...] = total[start - lower : start - lower + height]


def down_rows(place, pair_bits, masks, hidden, parts, other, n_out):
    rows, depth = hidden.shape
    width = sum(part.shape[1] for part in parts)
    return pl.pallas_call(
        functools.partial(down_kernel, pair_bits, masks, 1 if other is None else 0, n_out),
        out_shape=(jax.ShapeDtypeStruct((rows // 2 // n_out, width), jnp.bfloat16),) * n_out,
        in_specs=[SMEM, VMEM] + [HBM] * len(parts) + ([] if other is None else [VMEM]),
        out_specs=(VMEM,) * n_out,
        scratch_shapes=[
            pltpu.VMEM((depth, width), jnp.bfloat16),
            pltpu.SemaphoreType.DMA((len(parts),)),
        ],
        compiler_params=room(8),
        cost_estimate=pl.CostEstimate(flops=rows * width * depth, bytes_accessed=2 << 20, transcendentals=0),
    )(place, hidden, *parts, *([] if other is None else [other]))


def finish_kernel(pair_bits, plan, per_chunk, place_ref, middle_ref, *refs):
    out_ref = refs[-1]
    for chunk, (pair, span, strips, pitch, shift) in enumerate(plan):
        base = ((place_ref[0] >> pair_bits) ^ pair) * span
        totals = refs[chunk * per_chunk : (chunk + 1) * per_chunk]
        width = totals[0].shape[1] // strips
        for strip in range(strips):
            start = base + (strip * pitch + shift)
            cols = pl.ds(pl.multiple_of(start, width), width)
            total = middle_ref[:, cols]
            for ref in totals:
                total += ref[:, strip * width : (strip + 1) * width].astype(jnp.float32)
            out_ref[:, cols] = total.astype(jnp.bfloat16)


def finish(place, pair_bits, plan, middle, chunks):
    count = len(chunks) * len(chunks[0])
    return pl.pallas_call(
        functools.partial(finish_kernel, pair_bits, plan, len(chunks[0])),
        out_shape=jax.ShapeDtypeStruct(middle.shape, jnp.bfloat16),
        in_specs=[SMEM] + [VMEM] * (1 + count),
        out_specs=VMEM,
        compiler_params=room(8),
        cost_estimate=pl.CostEstimate(
            flops=8 * middle.size, bytes_accessed=8 * middle.size, transcendentals=0
        ),
    )(place, middle, *[block for chunk in chunks for block in chunk])


def lay_out(parts, starts, axis):
    total = sum(part.shape[axis] for part in parts)
    shape = list(parts[0].shape)
    shape[axis] = total
    whole = jnp.zeros(shape, parts[0].dtype)
    for part, start in zip(parts, starts):
        whole = lax.dynamic_update_slice_in_dim(whole, part, start, axis)
    return whole


def y_count(n_sp):
    return 1 << ((n_sp.bit_length() - 1) // 2)


def shards(q_proj, k_proj, v_proj, doc_ids, sinks, resid, w_out, norm_gain, w_gate, w_up, w_down):
    n_sp, n_tp = lax.axis_size("sp"), lax.axis_size("tp")
    n_y = y_count(n_sp)
    n_z = n_sp // n_y
    y_bits = n_y.bit_length() - 1
    place = jnp.stack([lax.axis_index("sp"), lax.axis_index("tp")]).astype(jnp.int32)
    depth, piece = w_gate.shape[0], w_down.shape[1]

    gu_cuts = 2 if depth % 32 == 0 else 1
    down_cuts = 2 if piece % 256 == 0 else 1
    step = depth // gu_cuts
    cuts = [(cut * step, (cut + 1) * step) for cut in range(gu_cuts)]
    wanted = [[(1, 0, depth), (0, *cuts[0]), (1, *cuts[0])], [(0, 0, depth)]]
    wanted[1] += [(parity, *cut) for cut in cuts[1:] for parity in (0, 1)]
    gu_half = {}
    for group in wanted:
        packed = pack_gate_up(place, y_bits, w_gate, w_up, tuple(group))
        for (parity, low, high), value in zip(group, packed):
            gu_half[parity, low, high] = value
    down_half = split_down(place, y_bits, w_down, down_cuts)

    gu = {}
    for dz in range(n_z):
        cuts = 1 if dz < 2 else gu_cuts
        height = depth // cuts
        for cut in range(cuts):
            held = swap(gu_half[dz % 2, cut * height, (cut + 1) * height], dz * n_y)
            for dy in range(n_y):
                start = (dz * n_y + dy, depth, cut * height)
                gu.setdefault(dz // 2, []).append((swap(held, dy), start))
    down, cuts_of = {}, {}
    for dz in range(n_z):
        cuts = cuts_of[dz // 2] = 1 if dz < 2 else down_cuts
        for cut in range(cuts):
            held = swap(down_half[dz % 2][cut + 1 if dz >= 2 else 0], dz * n_y)
            for dy in range(n_y):
                down[dz, cut, dy] = swap(held, dy)

    attended = attention(place, q_proj, k_proj, v_proj, doc_ids, sinks)

    out_blocks = {}
    for t in range(0, n_tp, 2):
        out_blocks[t] = swap(w_out, 0, t)
        out_blocks[t + 1] = swap(out_blocks[t], 0, 1)
    heads = [swap(attended[t], 0, t) for t in range(n_tp)]
    middle, normed = project(
        resid, norm_gain[None, :], heads, [out_blocks[t] for t in range(n_tp)]
    )

    rows = {(0, 0): normed, (1, 0): swap(normed, n_y)}
    for t in range(2, n_tp, 2):
        for a in (0, 1):
            rows[a, t] = swap(rows[a, 0], 0, t)
    for (a, t), block in list(rows.items()):
        rows[a, t + 1] = swap(block, 0, 1)
    order = [(a, t + c) for c in (0, 1) for a in (0, 1) for t in range(0, n_tp, 2)]

    blocks = [rows[key] for key in order]
    hidden = None
    for pairs in ([0], list(range(1, n_z // 2))):
        hidden = hidden_units(
            place,
            y_bits + 1,
            [(pair, [start for _, start in gu[pair]]) for pair in pairs],
            blocks,
            [[part for part, _ in gu[pair]] for pair in pairs],
            hidden,
            pairs[0] > 0,
        )

    span = 2 * n_y * piece
    plan, chunks = [], []
    for pair, cuts in cuts_of.items():
        width = piece // cuts
        for cut in range(cuts):
            keys = [(2 * pair + b, dy) for b in (0, 1) for dy in range(n_y)]
            masks = [dz * n_y + dy for dz, dy in keys]
            parts = [down[dz, cut, dy] for dz, dy in keys]
            if width % 128:
                starts = [((place[0] ^ mask) % (2 * n_y)) * width for mask in masks]
                parts, masks = [lay_out(parts, starts, 1)], [0]
            (sent,) = down_rows(place, y_bits + 1, masks, hidden, parts, None, 1)
            other = swap(sent, 0, 1)
            totals = down_rows(place, y_bits + 1, masks, hidden, parts, other, len(order) // 2)
            plan.append((pair, span) + ((1, span, 0) if cuts == 1 else (2 * n_y, piece, cut * width)))
            chunks.append([swap(totals[i], a * n_y, t) for i, (a, t) in enumerate(order[: len(order) // 2])])
    return finish(place, y_bits + 1, plan, middle, chunks)


def solution(mesh):
    placed = (
        P("sp", "tp"),
        P("sp", "tp"),
        P("sp", "tp"),
        P("sp"),
        P("tp"),
        P(("sp", "tp"), None),
        P("tp", None),
        P(),
        P("sp", "tp"),
        P("sp", "tp"),
        P("tp", "sp"),
    )

    return jax.shard_map(shards, mesh=mesh, in_specs=placed, out_specs=P(("sp", "tp"), None), check_vma=False)
```

```python
import functools

import jax
import jax.numpy as jnp
from jax import lax
from jax.experimental import pallas as pl
from jax.experimental.pallas import tpu as pltpu
from jax.sharding import PartitionSpec as P


HEAD = 64
WINDOW = 128

norm_eps = 1e-06
masked = -1e30


def swap(block, sp_mask=0, tp_mask=0):
    n_sp, n_tp = lax.axis_size("sp"), lax.axis_size("tp")
    if sp_mask and tp_mask:
        axis = ("sp", "tp")
        pairs = [
            (s * n_tp + t, (s ^ sp_mask) * n_tp + (t ^ tp_mask))
            for s in range(n_sp)
            for t in range(n_tp)
        ]
    elif sp_mask:
        axis, pairs = "sp", [(s, s ^ sp_mask) for s in range(n_sp)]
    elif tp_mask:
        axis, pairs = "tp", [(t, t ^ tp_mask) for t in range(n_tp)]
    else:
        return block
    return lax.ppermute(block, axis, pairs)


def edge_kernel(place_ref, docs_ref, k_ref, v_ref, *refs):
    kv_first_ref, kv_second_ref, doc_first_ref, doc_second_ref = refs[:4]
    for source, target in zip((docs_ref, k_ref, v_ref), refs[4:]):
        target[...] = source[...]
    even = place_ref[0] & 1 == 0
    last = k_ref.shape[0] - WINDOW
    kv_cols = k_ref.shape[1]
    for ref, cols in ((k_ref, slice(0, kv_cols)), (v_ref, slice(kv_cols, 2 * kv_cols))):
        head, tail = ref[:WINDOW, :], ref[last:, :]
        kv_first_ref[:, cols] = jnp.where(even, tail, head)
        kv_second_ref[:, cols] = jnp.where(even, head, tail)
    head, tail = docs_ref[:, :WINDOW], docs_ref[:, last:]
    doc_first_ref[...] = jnp.where(even, tail, head)
    doc_second_ref[...] = jnp.where(even, head, tail)


def attention_kernel(n_sp, n_out, place_ref, sinks_ref, docs_ref, q_ref, k_ref, v_ref, *refs):
    first_ref, second_ref, doc_first_ref, doc_second_ref = refs[:4]
    out_refs, attended = refs[4 : 4 + n_out], refs[4 + n_out]
    sp = place_ref[0]
    kv_cols = k_ref.shape[1]
    kv_heads = kv_cols // HEAD
    groups = q_ref.shape[1] // kv_cols
    count = q_ref.shape[0] // WINDOW
    span = 3 * WINDOW
    shape = (WINDOW, span)
    even = sp & 1 == 0
    offset = lax.broadcasted_iota(jnp.int32, shape, 1) - lax.broadcasted_iota(jnp.int32, shape, 0)
    near = (offset >= 0) & (offset <= 2 * WINDOW)
    ones = jnp.ones((span, HEAD), jnp.bfloat16)
    doc_first, doc_second = doc_first_ref[...], doc_second_ref[...]
    docs = jnp.concatenate(
        [
            jnp.where(sp == 0, -1, jnp.where(even, doc_second, doc_first)),
            docs_ref[...],
            jnp.where(sp == n_sp - 1, -1, jnp.where(even, doc_first, doc_second)),
        ],
        axis=1,
    )

    def band(own_ref, column, block):
        cols = slice(column, column + kv_cols)
        pieces = []
        for i in range(block - 1, block + 2):
            if 0 <= i < count:
                pieces.append(own_ref[i * WINDOW : (i + 1) * WINDOW, :])
            elif i < 0:
                pieces.append(jnp.where(even, second_ref[:, cols], first_ref[:, cols]))
            else:
                pieces.append(jnp.where(even, first_ref[:, cols], second_ref[:, cols]))
        return jnp.concatenate(pieces, axis=0)

    for block in range(count):
        rows = slice(block * WINDOW, (block + 1) * WINDOW)
        own_docs = docs[:, (block + 1) * WINDOW : (block + 2) * WINDOW]
        query_docs = jnp.broadcast_to(own_docs, (WINDOW, WINDOW)).T
        band_docs = docs[:, block * WINDOW : block * WINDOW + span]
        valid = near & (jnp.concatenate([query_docs] * 3, axis=1) == band_docs)
        keys, values = band(k_ref, 0, block), band(v_ref, kv_cols, block)
        queries = q_ref[rows, :] * HEAD ** (-0.5)
        outs = []
        for head in range(kv_heads):
            cols = slice(head * HEAD, (head + 1) * HEAD)
            key = keys[:, cols]
            value = jnp.concatenate([values[:, cols], ones], axis=1)
            for group in range(groups):
                index = head * groups + group
                scores = lax.dot_general(
                    queries[:, index * HEAD : (index + 1) * HEAD],
                    key,
                    (((1,), (1,)), ((), ())),
                    preferred_element_type=jnp.float32,
                )
                scores = jnp.where(valid, scores, masked)
                sink = sinks_ref[index]
                top = jnp.maximum(jnp.max(scores, axis=-1, keepdims=True), sink)
                expd = jnp.exp(scores - top).astype(jnp.bfloat16)
                both = jnp.dot(expd, value, preferred_element_type=jnp.float32)
                outs.append(both[:, :HEAD] / (both[:, HEAD:] + jnp.exp(sink - top)))
        attended[rows, :] = jnp.concatenate(outs, axis=1).astype(jnp.bfloat16)
    height = out_refs[0].shape[0]
    for i, out_ref in enumerate(out_refs):
        out_ref[...] = attended[pl.ds(pl.multiple_of((place_ref[1] ^ i) * height, height), height), :]


def attention(place, q_proj, k_proj, v_proj, doc_ids, sinks):
    tok_rows, kv_cols = k_proj.shape
    n_tp, n_sp = lax.axis_size("tp"), lax.axis_size("sp")
    doc_ids = doc_ids[None, :]
    kv_edge = jax.ShapeDtypeStruct((WINDOW, 2 * kv_cols), jnp.bfloat16)
    doc_edge = jax.ShapeDtypeStruct((1, WINDOW), jnp.int32)
    same = [jax.ShapeDtypeStruct(array.shape, array.dtype) for array in (doc_ids, k_proj, v_proj)]
    kv_first, kv_second, doc_first, doc_second, doc_ids, k_proj, v_proj = pl.pallas_call(
        edge_kernel,
        out_shape=(kv_edge, kv_edge, doc_edge, doc_edge, *same),
        in_specs=[SMEM] + [VMEM] * 3,
        out_specs=(VMEM,) * 7,
        compiler_params=room(4),
    )(place, doc_ids, k_proj, v_proj)

    def trade(name, block):
        low = int(name.endswith("second"))
        pairs = [(i, i + 1) for i in range(low, n_sp - 1, 2)]
        return lax.ppermute(block, "sp", pairs + [(b, a) for a, b in pairs])

    edges = [trade("kv_first", kv_first), trade("kv_second", kv_second)]
    edges += [trade("doc_first", doc_first), trade("doc_second", doc_second)]
    own = jax.ShapeDtypeStruct((tok_rows // n_tp, q_proj.shape[1]), jnp.bfloat16)
    return pl.pallas_call(
        functools.partial(attention_kernel, n_sp, n_tp),
        out_shape=(own,) * n_tp,
        in_specs=[SMEM] * 2 + [VMEM] * 8,
        out_specs=(VMEM,) * n_tp,
        scratch_shapes=[pltpu.VMEM(q_proj.shape, jnp.bfloat16)],
        compiler_params=room(8),
        cost_estimate=pl.CostEstimate(
            flops=12 * tok_rows * WINDOW * q_proj.shape[1],
            bytes_accessed=1 << 20,
            transcendentals=0,
        ),
    )(place, sinks, doc_ids, q_proj, k_proj, v_proj, *edges)


SMEM = pl.BlockSpec(memory_space=pltpu.SMEM)
VMEM = pl.BlockSpec(memory_space=pltpu.VMEM)
ANY = pl.BlockSpec(memory_space=pl.ANY)
HBM = pl.BlockSpec(memory_space=pltpu.HBM)


def room(mebibytes):
    return pltpu.CompilerParams(vmem_limit_bytes=mebibytes << 20)


def pack_kernel(half, y_bits, wanted, place_ref, gate_ref, up_ref, *refs):
    whole = half // 128 * 128

    def fill(source, chosen):
        lower = source * half

        def store(start, value):
            for (_, low, high), ref in chosen:
                ref[:, start : start + value.shape[1]] = value[low:high]

        for start in range(0, whole, 128):
            for ref, shift in ((gate_ref, 0), (up_ref, 128)):
                store(2 * start + shift, ref[:, lower + start : lower + start + 128])
        if half > whole:
            rest = [ref[:, lower + whole : lower + half] for ref in (gate_ref, up_ref)]
            store(2 * whole, jnp.concatenate(rest, axis=1))

    for source in (0, 1):
        for parity in (0, 1):
            chosen = [(want, ref) for want, ref in zip(wanted, refs) if want[0] == parity]

            @pl.when((place_ref[0] >> y_bits) & 1 == source ^ parity)
            def _():
                fill(source, chosen)


def pack_gate_up(place, y_bits, w_gate, w_up, wanted):
    depth, width = w_gate.shape
    return pl.pallas_call(
        functools.partial(pack_kernel, width // 2, y_bits, wanted),
        out_shape=tuple(
            jax.ShapeDtypeStruct((high - low, width), jnp.bfloat16) for _, low, high in wanted
        ),
        in_specs=[SMEM, VMEM, VMEM],
        out_specs=(VMEM,) * len(wanted),
        compiler_params=room(8),
        cost_estimate=pl.CostEstimate(flops=4 * depth * width, bytes_accessed=6 * w_gate.size, transcendentals=0),
    )(place, w_gate, w_up)


def split_kernel(y_bits, place_ref, down_ref, *refs):
    half = refs[0].shape[0]
    for parity, ref in enumerate(refs):
        lower = pl.multiple_of(((place_ref[0] >> y_bits) & 1 ^ parity) * half, half)
        ref[...] = down_ref[pl.ds(lower, half), :]


def split_down(place, y_bits, w_down):
    depth, width = w_down.shape
    return pl.pallas_call(
        functools.partial(split_kernel, y_bits),
        out_shape=(jax.ShapeDtypeStruct((depth // 2, width), jnp.bfloat16),) * 2,
        in_specs=[SMEM, VMEM],
        out_specs=(VMEM,) * 2,
        compiler_params=room(8),
        cost_estimate=pl.CostEstimate(flops=depth * width, bytes_accessed=8 * depth * width, transcendentals=0),
    )(place, w_down)


def project_kernel(count, resid_ref, gain_ref, *refs):
    heads, weights, (middle_ref, normed_ref) = refs[:count], refs[count : 2 * count], refs[2 * count :]
    width = middle_ref.shape[1]
    tile = min(512, width)
    squares = jnp.zeros((middle_ref.shape[0], 1), jnp.float32)
    for lower in range(0, width, tile):
        cols = pl.ds(lower, tile)
        total = resid_ref[:, cols].astype(jnp.float32)
        for head, weight in zip(heads, weights):
            total += jnp.dot(head[...], weight[:, cols], preferred_element_type=jnp.float32)
        middle_ref[:, cols] = total
        squares += jnp.sum(total * total, axis=-1, keepdims=True)
    factor = lax.rsqrt(squares / width + norm_eps)
    for lower in range(0, width, tile):
        cols = pl.ds(lower, tile)
        normed_ref[:, cols] = (middle_ref[:, cols] * factor * gain_ref[:, cols]).astype(jnp.bfloat16)


def project(resid, gain, heads, weights):
    rows, width = resid.shape
    count = len(heads)
    return pl.pallas_call(
        functools.partial(project_kernel, count),
        out_shape=(
            jax.ShapeDtypeStruct((rows, width), jnp.float32),
            jax.ShapeDtypeStruct((rows, width), jnp.bfloat16),
        ),
        in_specs=[VMEM] * (2 + 2 * count),
        out_specs=(VMEM, VMEM),
        compiler_params=room(12),
        cost_estimate=pl.CostEstimate(
            flops=2 * rows * width * count * heads[0].shape[1], bytes_accessed=6 << 20, transcendentals=0
        ),
    )(resid, gain, *heads, *weights)


def hidden_kernel(n_rows, pair_bits, groups, with_total, last, place_ref, *refs):
    counts = [len(starts) for _, starts in groups]
    row_refs, refs = refs[:n_rows], refs[n_rows:]
    part_refs, refs = refs[: sum(counts)], refs[sum(counts) :]
    if with_total:
        total_ref, refs = refs[0], refs[1:]
    out_ref, rows, weight, row_sems, part_sems = refs
    pairs, span = len(counts), weight.shape[1]
    height = row_refs[0].shape[0]
    row_copies, part_copies = [], []
    index = 0
    for pair, count in enumerate(counts):
        columns = pl.ds(pl.multiple_of(((place_ref[0] >> pair_bits) ^ groups[pair][0]) * span, span), span)
        for i, ref in enumerate(row_refs):
            row_copies.append(
                pltpu.make_async_copy(
                    ref.at[:, columns], rows.at[pair, pl.ds(i * height, height)], row_sems.at[pair, i]
                )
            )
        for (mask, scale, shift), ref in zip(groups[pair][1], part_refs[index : index + count]):
            within = (place_ref[0] ^ mask) & ((1 << pair_bits) - 1)
            start = pl.multiple_of(within * scale + shift, ref.shape[0])
            part_copies.append(
                pltpu.make_async_copy(ref, weight.at[pair, pl.ds(start, ref.shape[0])], part_sems.at[index])
            )
            index += 1
    for copy in part_copies + row_copies:
        copy.start()
    for copy in part_copies:
        copy.wait()
    total_rows, width = rows.shape[1], weight.shape[2]
    tile = min(512, total_rows)
    for lower in range(0, total_rows, tile):
        part = pl.ds(lower, tile)
        for i in range(lower // height, (lower + tile) // height):
            for pair in range(pairs):
                row_copies[pair * n_rows + i].wait()
        for start in range(0, width, 256):
            size = min(256, width - start)
            cols = slice(start, start + size)
            both = total_ref[part, cols] if with_total else 0.0
            for pair in range(pairs):
                both += jnp.dot(rows[pair, part, :], weight[pair, :, cols], preferred_element_type=jnp.float32)
            if last:
                gate, up = both[:, : size // 2], both[:, size // 2 :]
                out_ref[part, start // 2 : (start + size) // 2] = (gate / (1.0 + jnp.exp(-gate)) * up).astype(
                    jnp.bfloat16
                )
            else:
                out_ref[part, cols] = both


def hidden_units(place, pair_bits, groups, row_blocks, parts, total, last):
    rows = sum(block.shape[0] for block in row_blocks)
    width = parts[0][0].shape[1]
    span = sum(part.shape[0] for part in parts[0])
    flat = [part for group in parts for part in group]
    out = jax.ShapeDtypeStruct((rows, width // 2), jnp.bfloat16)
    if not last:
        out = jax.ShapeDtypeStruct((rows, width), jnp.float32)
    return pl.pallas_call(
        functools.partial(
            hidden_kernel, len(row_blocks), pair_bits, groups, total is not None, last
        ),
        out_shape=out,
        in_specs=[SMEM]
        + [HBM] * (len(row_blocks) + len(flat))
        + ([VMEM] if total is not None else []),
        out_specs=VMEM,
        scratch_shapes=[
            pltpu.VMEM((len(parts), rows, span), jnp.bfloat16),
            pltpu.VMEM((len(parts), span, width), jnp.bfloat16),
            pltpu.SemaphoreType.DMA((len(parts), len(row_blocks))),
            pltpu.SemaphoreType.DMA((len(flat),)),
        ],
        cost_estimate=pl.CostEstimate(
            flops=2 * rows * width * span * len(parts),
            bytes_accessed=8 << 20,
            transcendentals=0,
        ),
        compiler_params=room(12),
    )(place, *row_blocks, *flat, *([total] if total is not None else []))


def down_kernel(skip_bits, pair_bits, masks, base, n_out, place_ref, hidden_ref, *refs):
    part_refs, refs = refs[: len(masks)], refs[len(masks) :]
    other_ref, refs = (refs[0], refs[1:]) if n_out > 1 else (None, refs)
    out_refs, (weight, sems) = refs[:n_out], refs[n_out:]
    copies = []
    for i, ref in enumerate(part_refs):
        start = 0
        if len(masks) > 1:
            within = ((place_ref[0] ^ masks[i]) & ((1 << pair_bits) - 1)) >> skip_bits
            start = pl.multiple_of(within * ref.shape[1], ref.shape[1])
        copies.append(pltpu.make_async_copy(ref, weight.at[:, pl.ds(start, ref.shape[1])], sems.at[i]))
    for copy in copies:
        copy.start()
    for copy in copies:
        copy.wait()
    rows = hidden_ref.shape[0] // 2
    height = rows // n_out
    tile = min(256, rows)
    for lower in range(0, rows, tile):
        total = jnp.dot(
            hidden_ref[pl.ds(base * rows + lower, tile), :], weight[...], preferred_element_type=jnp.float32
        )
        if n_out == 1:
            out_refs[0][pl.ds(lower, tile), :] = total.astype(jnp.bfloat16)
            continue
        total = (total + other_ref[pl.ds(lower, tile), :].astype(jnp.float32)).astype(jnp.bfloat16)
        for start in range(lower, lower + tile, height):
            out_refs[start // height][...] = total[start - lower : start - lower + height]


def down_rows(place, skip_bits, pair_bits, masks, hidden, parts, other, n_out):
    rows, depth = hidden.shape
    width = sum(part.shape[1] for part in parts)
    return pl.pallas_call(
        functools.partial(down_kernel, skip_bits, pair_bits, masks, 1 if other is None else 0, n_out),
        out_shape=(jax.ShapeDtypeStruct((rows // 2 // n_out, width), jnp.bfloat16),) * n_out,
        in_specs=[SMEM, VMEM] + [HBM] * len(parts) + ([] if other is None else [VMEM]),
        out_specs=(VMEM,) * n_out,
        scratch_shapes=[
            pltpu.VMEM((depth, width), jnp.bfloat16),
            pltpu.SemaphoreType.DMA((len(parts),)),
        ],
        compiler_params=room(8),
        cost_estimate=pl.CostEstimate(flops=rows * width * depth, bytes_accessed=2 << 20, transcendentals=0),
    )(place, hidden, *parts, *([] if other is None else [other]))


def finish_kernel(pair_bits, plan, per_chunk, place_ref, middle_ref, *refs):
    out_ref = refs[-1]
    for chunk, (pair, span, strips, dy) in enumerate(plan):
        base = ((place_ref[0] >> pair_bits) ^ pair) * span
        pitch = span // strips
        shift = 0 if dy is None else ((place_ref[0] & ((1 << pair_bits - 1) - 1)) ^ dy) * (pitch >> pair_bits - 1)
        totals = refs[chunk * per_chunk : (chunk + 1) * per_chunk]
        width = totals[0].shape[1] // strips
        for strip in range(strips):
            start = base + (strip * pitch + shift)
            cols = pl.ds(pl.multiple_of(start, width), width)
            total = middle_ref[:, cols]
            for ref in totals:
                total += ref[:, strip * width : (strip + 1) * width].astype(jnp.float32)
            out_ref[:, cols] = total.astype(jnp.bfloat16)


def finish(place, pair_bits, plan, middle, chunks):
    count = len(chunks) * len(chunks[0])
    return pl.pallas_call(
        functools.partial(finish_kernel, pair_bits, plan, len(chunks[0])),
        out_shape=jax.ShapeDtypeStruct(middle.shape, jnp.bfloat16),
        in_specs=[SMEM] + [VMEM] * (1 + count),
        out_specs=VMEM,
        compiler_params=room(8),
        cost_estimate=pl.CostEstimate(
            flops=8 * middle.size, bytes_accessed=8 * middle.size, transcendentals=0
        ),
    )(place, middle, *[block for chunk in chunks for block in chunk])


def lay_out(parts, starts, axis):
    total = sum(part.shape[axis] for part in parts)
    shape = list(parts[0].shape)
    shape[axis] = total
    whole = jnp.zeros(shape, parts[0].dtype)
    for part, start in zip(parts, starts):
        whole = lax.dynamic_update_slice_in_dim(whole, part, start, axis)
    return whole


def y_count(n_sp):
    return 1 << ((n_sp.bit_length() - 1) // 2)


def shards(q_proj, k_proj, v_proj, doc_ids, sinks, resid, w_out, norm_gain, w_gate, w_up, w_down):
    n_sp, n_tp = lax.axis_size("sp"), lax.axis_size("tp")
    n_y = y_count(n_sp)
    n_z = n_sp // n_y
    y_bits = n_y.bit_length() - 1
    place = jnp.stack([lax.axis_index("sp"), lax.axis_index("tp")]).astype(jnp.int32)
    depth, piece = w_gate.shape[0], w_down.shape[1]

    gu_cuts = 2 if depth % 32 == 0 else 1
    step = depth // gu_cuts
    cuts = [(cut * step, (cut + 1) * step) for cut in range(gu_cuts)]
    wanted = [[(1, 0, depth), (0, *cuts[0]), (1, *cuts[0])], [(0, 0, depth)]]
    wanted[1] += [(parity, *cut) for cut in cuts[1:] for parity in (0, 1)]
    gu_half = {}
    for group in wanted:
        packed = pack_gate_up(place, y_bits, w_gate, w_up, tuple(group))
        for (parity, low, high), value in zip(group, packed):
            gu_half[parity, low, high] = value
    down_half = split_down(place, y_bits, w_down)

    gu = {}
    for dz in range(n_z):
        cuts = 1 if dz < 2 else gu_cuts
        height = depth // cuts
        for cut in range(cuts):
            held = swap(gu_half[dz % 2, cut * height, (cut + 1) * height], dz * n_y)
            for dy in range(n_y):
                start = (dz * n_y + dy, depth, cut * height)
                gu.setdefault(dz // 2, []).append((swap(held, dy), start))
    down = {}
    for dz in range(n_z):
        held = swap(down_half[dz % 2], dz * n_y)
        for dy in range(n_y):
            down[dz, dy] = swap(held, dy)

    attended = attention(place, q_proj, k_proj, v_proj, doc_ids, sinks)

    out_blocks = {}
    for t in range(0, n_tp, 2):
        out_blocks[t] = swap(w_out, 0, t)
        out_blocks[t + 1] = swap(out_blocks[t], 0, 1)
    heads = [swap(attended[t], 0, t) for t in range(n_tp)]
    middle, normed = project(
        resid, norm_gain[None, :], heads, [out_blocks[t] for t in range(n_tp)]
    )

    rows = {(0, 0): normed, (1, 0): swap(normed, n_y)}
    for t in range(2, n_tp, 2):
        for a in (0, 1):
            rows[a, t] = swap(rows[a, 0], 0, t)
    for (a, t), block in list(rows.items()):
        rows[a, t + 1] = swap(block, 0, 1)
    order = [(a, t + c) for c in (0, 1) for a in (0, 1) for t in range(0, n_tp, 2)]

    blocks = [rows[key] for key in order]
    hidden = None
    for pairs in ([0], list(range(1, n_z // 2))):
        hidden = hidden_units(
            place,
            y_bits + 1,
            [(pair, [start for _, start in gu[pair]]) for pair in pairs],
            blocks,
            [[part for part, _ in gu[pair]] for pair in pairs],
            hidden,
            pairs[0] > 0,
        )

    span = 2 * n_y * piece
    plan, chunks = [], []
    for pair in range(n_z // 2):
        groups = [[dy] for dy in range(n_y)] if pair and piece % 128 == 0 else [list(range(n_y))]
        for group in groups:
            keys = [(2 * pair + b, dy) for b in (0, 1) for dy in group]
            masks = [dz * n_y + dy for dz, dy in keys]
            parts = [down[key] for key in keys]
            if piece % 128:
                starts = [((place[0] ^ mask) % (2 * n_y)) * piece for mask in masks]
                parts, masks = [lay_out(parts, starts, 1)], [0]
            skip = y_bits if len(groups) > 1 else 0
            (sent,) = down_rows(place, skip, y_bits + 1, masks, hidden, parts, None, 1)
            other = swap(sent, 0, 1)
            totals = down_rows(place, skip, y_bits + 1, masks, hidden, parts, other, len(order) // 2)
            plan.append((pair, span, 2, group[0]) if len(groups) > 1 else (pair, span, 1, None))
            chunks.append([swap(totals[i], a * n_y, t) for i, (a, t) in enumerate(order[: len(order) // 2])])
    return finish(place, y_bits + 1, plan, middle, chunks)


def solution(mesh):
    placed = (
        P("sp", "tp"),
        P("sp", "tp"),
        P("sp", "tp"),
        P("sp"),
        P("tp"),
        P(("sp", "tp"), None),
        P("tp", None),
        P(),
        P("sp", "tp"),
        P("sp", "tp"),
        P("tp", "sp"),
    )

    return jax.shard_map(shards, mesh=mesh, in_specs=placed, out_specs=P(("sp", "tp"), None), check_vma=False)
```
